256 devices in a mesh: sp: 32 (over z, x), tp: 8 (over y, core).
Axes of the slice: x: 4, y: 4, z: 8, core: 2. Of those that a mesh axis runs over, the one named last changes fastest.
Arguments:
- tokens: bfloat16 [8192, 4096], P('sp', 'tp'), may hold values from -6 to 6
- norm_gain: float32 [4096], replicated, may hold values from 0.1 to 1.9
- fox_query: bfloat16 [4096, 1024], P(None, 'tp'), may hold values from -0.234375 to 0.234375
- fox_key: bfloat16 [4096, 1024], P(None, 'tp'), may hold values from -0.09375 to 0.09375
- fox_value: bfloat16 [4096, 1024], P(None, 'tp'), may hold values from -0.09375 to 0.09375
- cum_gate: float32 [8, 8192], P('tp'), as said below
- lin_query: bfloat16 [4096, 1024], P(None, 'tp'), may hold values from -0.09375 to 0.09375
- lin_key: bfloat16 [4096, 1024], P(None, 'tp'), may hold values from -0.09375 to 0.09375
- lin_value: bfloat16 [4096, 2048], P(None, 'tp'), may hold values from -0.09375 to 0.09375
- decay_down: bfloat16 [4096, 16], replicated, may hold values from -0.09375 to 0.09375
- decay_up: bfloat16 [16, 1024], P(None, 'tp'), may hold values from -1.5 to 1.5
- decay_bias: float32 [1024], P('tp'), may hold values from 0.5 to 11
- lin_gain: float32 [256], replicated, may hold values from 0.1 to 1.9
- fox_out: bfloat16 [1024, 4096], P('tp'), may hold values from -0.109375 to 0.109375
- lin_out: bfloat16 [2048, 4096], P('tp'), may hold values from -0.109375 to 0.109375
Outputs:
- mixed: bfloat16 [8192, 4096], P(('sp', 'tp'))
- log_total: float32 [8, 8192], P('tp', 'sp')
The draws below stay inside these ranges and needn't reach their ends.
Inputs may be any that keep to these rules, and one draw needn't show every extreme that they name: `cum_gate`: along positions each head's values never rise.
All inputs are finite; a program needn't handle non-finite values.
Results may differ from the reference program's by a relative error of at most 0.017.
Values may be sent and summed in bfloat16 or wider, within the bound.
A program may use at most 64 MiB of HBM per device.

```python
import math
import jax
import jax.numpy as jnp
from jax import lax

D = 4096
HEAD = 128
FOX_HEADS = 8
LIN_HEADS = 8
KEY_DIM = 128
VAL_DIM = 256
RANK = 16
BLOCK = 64
TOK_DEV = 256
TOKENS = 8192
N_TP = 8


def base_projection(key, salt, spread):
    bound = 6.0 * spread * D ** (-0.5)
    base = jax.random.normal(jax.random.fold_in(key, salt), (D, FOX_HEADS * HEAD), jnp.float32) * spread * D ** (-0.5)
    return jnp.clip(base, -bound, bound)


def draw_fox_query(key, part):
    base = base_projection(key, 31, 2.5)
    return base.astype(jnp.bfloat16)


def draw_fox_key(key, part):
    base = base_projection(key, 37, 1.0)
    return base.astype(jnp.bfloat16)


def draw_tokens(key, part):
    noise = jax.random.normal(jax.random.fold_in(key, 43), (TOKENS, D), jnp.float32)
    return jnp.clip(noise, -6.0, 6.0).astype(jnp.bfloat16)


def draw_cum_gate(key, part):
    keys = jax.random.split(jax.random.fold_in(key, 11), 5)
    order = jax.random.permutation(keys[0], FOX_HEADS)
    gradual_decline = order < FOX_HEADS // 2
    rate = jnp.where(gradual_decline, 0.5 / TOKENS, 1.0 / 50.0)
    factor = jnp.exp(jax.random.uniform(keys[1], (FOX_HEADS, TOKENS // TOK_DEV), jnp.float32, -0.9, 0.9))
    factor = jnp.repeat(factor, TOK_DEV, axis=1)
    noise = jax.random.uniform(keys[2], (FOX_HEADS, TOKENS), jnp.float32, 0.3, 1.7)
    update_rounds = -rate[:, None] * factor * noise
    spots = jax.random.randint(keys[3], (FOX_HEADS, 3), 0, TOKENS)
    removed_entries = jax.random.uniform(keys[4], (FOX_HEADS, 3), jnp.float32, 0.22, 0.69)
    matched_entries = jnp.arange(TOKENS)[None, None, :] == spots[:, :, None]
    sudden_spike = jnp.sum(jnp.where(matched_entries, removed_entries[:, :, None], 0.0), axis=1)
    update_rounds = update_rounds - jnp.where(gradual_decline[:, None], sudden_spike, 0.0)
    return jnp.cumsum(update_rounds, axis=1)


def draw_decay_bias(key, part):
    keys = jax.random.split(jax.random.fold_in(key, 23), 2)
    order = jax.random.permutation(keys[0], LIN_HEADS)
    gradual_decline = order < LIN_HEADS // 2
    lower = jnp.where(gradual_decline, 9.0, 0.5)
    upper = jnp.where(gradual_decline, 11.0, 1.5)
    fraction = jax.random.uniform(keys[1], (LIN_HEADS, KEY_DIM), jnp.float32)
    return (lower[:, None] + (upper - lower)[:, None] * fraction).reshape(LIN_HEADS * KEY_DIM)


def shard_levels(key, shape, cuts, low, top_value):
    level, own = 1.0, jax.random.fold_in(key, 6)
    for position, blocks in cuts:
        steps = jnp.exp(jax.random.uniform(jax.random.fold_in(own, position), (blocks,), jnp.float32, low / len(cuts), top_value / len(cuts)))
        level = level * jnp.repeat(steps, shape[position] // blocks).reshape([-1 if axis == position else 1 for axis in range(len(shape))])
    return level


def centred(rng, extent, scale, limit, shards=(), held_as=jnp.bfloat16):
    factor_of = shard_levels(rng, extent, shards, -0.22, 0.18) if shards else 1.0
    result = jax.random.normal(rng, extent, jnp.float32) * scale * factor_of
    return jnp.minimum(jnp.maximum(result, -limit), limit).astype(held_as)


def setup_inputs(seed: int = 0) -> dict:
    seeds = jax.random.split(jax.random.key(seed), 16)
    tokens = draw_tokens(jax.random.fold_in(seeds[15], 71), 0)
    norm_gain = jnp.clip(1.0 + 0.18 * jax.random.normal(seeds[1], (D,), jnp.float32), 0.1, 1.9)
    fox_query = draw_fox_query(jax.random.fold_in(seeds[15], 71), 0)
    fox_key = draw_fox_key(jax.random.fold_in(seeds[15], 71), 0)
    fox_value = centred(seeds[4], (D, FOX_HEADS * HEAD), D ** -0.5, 0.09375, ((1, 8),))
    cum_gate = draw_cum_gate(jax.random.fold_in(seeds[15], 71), 0)
    lin_query = centred(seeds[6], (D, LIN_HEADS * KEY_DIM), D ** -0.5, 0.09375, ((1, 8),))
    lin_key = centred(seeds[7], (D, LIN_HEADS * KEY_DIM), D ** -0.5, 0.09375, ((1, 8),))
    lin_value = centred(seeds[8], (D, LIN_HEADS * VAL_DIM), D ** -0.5, 0.09375, ((1, 8),))
    decay_down = centred(seeds[9], (D, RANK), D ** -0.5, 0.09375)
    decay_up = centred(seeds[10], (RANK, LIN_HEADS * KEY_DIM), RANK ** -0.5, 1.5, ((1, 8),))
    decay_bias = draw_decay_bias(jax.random.fold_in(seeds[15], 71), 0)
    lin_gain = jnp.clip(1.0 + 0.18 * jax.random.normal(seeds[12], (VAL_DIM,), jnp.float32), 0.1, 1.9)
    fox_out = centred(seeds[13], (FOX_HEADS * HEAD, D), (FOX_HEADS * HEAD + LIN_HEADS * VAL_DIM) ** -0.5, 0.109375, ((0, 8),))
    lin_out = centred(seeds[14], (LIN_HEADS * VAL_DIM, D), (FOX_HEADS * HEAD + LIN_HEADS * VAL_DIM) ** -0.5, 0.109375, ((0, 8),))
    return dict(tokens=tokens, norm_gain=norm_gain, fox_query=fox_query, fox_key=fox_key, fox_value=fox_value, cum_gate=cum_gate, lin_query=lin_query, lin_key=lin_key, lin_value=lin_value, decay_down=decay_down, decay_up=decay_up, decay_bias=decay_bias, lin_gain=lin_gain, fox_out=fox_out, lin_out=lin_out)


EPS = 1e-06
TAU = 16.0

def rms_scale(values, gain):
    return values * lax.rsqrt(lax.optimization_barrier(jnp.mean(values * values, axis=-1, keepdims=True)) + EPS) * gain

def block_step(state, q_b, k_b, v_b, cum):
    high = lax.Precision.HIGHEST
    inter = jnp.dot(q_b * jnp.exp(cum), state, precision=high)
    span = cum.shape[0]
    causal = jnp.arange(span)[:, None] >= jnp.arange(span)[None, :]
    rel = cum[:, None, :] - cum[None, :, :]
    decay = jnp.exp(jnp.where(causal[:, :, None], rel, -jnp.inf))
    scores = jnp.einsum('id,jd,ijd->ij', q_b, k_b, decay, precision=high)
    intra = jnp.dot(scores, v_b, precision=high)
    last = cum[-1]
    new_state = jnp.exp(last)[:, None] * state + jnp.dot((k_b * jnp.exp(last[None, :] - cum)).T, v_b, precision=high)
    return (new_state, inter + intra)

def linear_head(q, k, v, g):
    count = TOKENS // BLOCK

    def step(state, item):
        q_b, k_b, v_b, g_b = item
        return block_step(state, q_b, k_b, v_b, jnp.cumsum(g_b, axis=0))
    items = (q.reshape(count, BLOCK, KEY_DIM), k.reshape(count, BLOCK, KEY_DIM), v.reshape(count, BLOCK, VAL_DIM), g.reshape(count, BLOCK, KEY_DIM))
    _, out = lax.scan(step, jnp.zeros((KEY_DIM, VAL_DIM), jnp.float32), items)
    return out.reshape(TOKENS, VAL_DIM)

def fox_head(q, k, v, cum):
    rows = math.gcd(TOKENS, 512)
    scale = HEAD ** (-0.5)
    key_pos = jnp.arange(TOKENS, dtype=jnp.int32)

    def one(index):
        start = index * rows
        q_i = lax.dynamic_slice_in_dim(q, start, rows, 0)
        c_i = lax.dynamic_slice_in_dim(cum, start, rows, 0)
        logits = jnp.dot(q_i, k.T, preferred_element_type=jnp.float32) * scale + (c_i[:, None] - cum[None, :])
        q_pos = start + jnp.arange(rows, dtype=jnp.int32)
        logits = jnp.where(key_pos[None, :] <= q_pos[:, None], logits, -jnp.inf)
        top = lax.optimization_barrier(jnp.max(logits, axis=1))
        weights = jnp.exp(logits - top[:, None])
        total = lax.optimization_barrier(jnp.sum(weights, axis=1))
        heads = jnp.dot(weights.astype(jnp.bfloat16), v, preferred_element_type=jnp.float32) / total[:, None]
        return (heads.astype(jnp.bfloat16), top + jnp.log(total))
    heads, logs = lax.map(one, jnp.arange(TOKENS // rows, dtype=jnp.int32))
    return (heads.reshape(TOKENS, HEAD), logs.reshape(TOKENS))

def split_heads(values, count):
    return values.reshape(TOKENS, count, values.shape[1] // count).transpose(1, 0, 2)

def reference(tokens, norm_gain, fox_query, fox_key, fox_value, cum_gate, lin_query, lin_key, lin_value, decay_down, decay_up, decay_bias, lin_gain, fox_out, lin_out):
    normed = rms_scale(tokens.astype(jnp.float32), norm_gain).astype(jnp.bfloat16)

    def project(weight):
        return jnp.dot(normed, weight, preferred_element_type=jnp.float32).astype(jnp.bfloat16)
    fq = split_heads(project(fox_query), FOX_HEADS)
    fk = split_heads(project(fox_key), FOX_HEADS)
    fv = split_heads(project(fox_value), FOX_HEADS)
    fox_heads, log_total = lax.map(lambda item: fox_head(*item), (fq, fk, fv, cum_gate))
    fox_flat = fox_heads.transpose(1, 0, 2).reshape(TOKENS, FOX_HEADS * HEAD)
    lq = project(lin_query).astype(jnp.float32) * KEY_DIM ** (-0.5)
    lk = project(lin_key).astype(jnp.float32)
    lv = project(lin_value).astype(jnp.float32)
    low = project(decay_down)
    log_decay = jax.nn.log_sigmoid(jnp.dot(low, decay_up, preferred_element_type=jnp.float32) + decay_bias) / TAU
    lin_raw = jax.vmap(linear_head)(split_heads(lq, LIN_HEADS), split_heads(lk, LIN_HEADS), split_heads(lv, LIN_HEADS), split_heads(log_decay, LIN_HEADS))
    lin_heads = rms_scale(lin_raw, lin_gain).astype(jnp.bfloat16)
    lin_flat = lin_heads.transpose(1, 0, 2).reshape(TOKENS, LIN_HEADS * VAL_DIM)
    fox_group = FOX_HEADS // N_TP * HEAD
    lin_group = LIN_HEADS // N_TP * VAL_DIM
    total = jnp.zeros((TOKENS, D), jnp.float32)
    for group in range(N_TP):
        part = jnp.dot(fox_flat[:, group * fox_group:(group + 1) * fox_group], fox_out[group * fox_group:(group + 1) * fox_group], preferred_element_type=jnp.float32)
        part = part + jnp.dot(lin_flat[:, group * lin_group:(group + 1) * lin_group], lin_out[group * lin_group:(group + 1) * lin_group], preferred_element_type=jnp.float32)
        total = total + lax.optimization_barrier(part.astype(jnp.bfloat16)).astype(jnp.float32)
    return (total.astype(jnp.bfloat16), log_total)
```

```python
import jax
import jax.numpy as jnp
from jax import lax
from jax.experimental import pallas as pl
from jax.experimental.pallas import tpu as pltpu
from jax.sharding import Mesh
from jax.sharding import PartitionSpec as P

MESH = pl.DeviceIdType.MESH
F32 = jnp.float32
BF16 = jnp.bfloat16

NZ, NX, NY, NC = 8, 4, 4, 2
TOK = 256
D = 4096
FEAT = 512
HEAD = 128
VAL = 256
EPS = 1e-06
TAU = 16.0
LOW = -3.0e38
KEY_SCALE = 128 ** (-0.5)

CHUNKS = 4
ROWS = TOK // CHUNKS
KV_CHUNKS = 4
KV_ROWS = TOK // KV_CHUNKS
COL_CHUNKS = 8
COLS = D // COL_CHUNKS
N_SEM = 160
N_LOC = 16


def nt(a, b):
    return lax.dot_general(a, b, (((1,), (1,)), ((), ())), preferred_element_type=F32)


def tn(a, b):
    return lax.dot_general(a, b, (((0,), (0,)), ((), ())), preferred_element_type=F32)


def mm(a, b):
    return jnp.dot(a, b, preferred_element_type=F32)


def iota(shape, dim):
    return lax.broadcasted_iota(jnp.int32, shape, dim)


def column_of(row):
    eye = iota((128, 128), 0) == iota((128, 128), 1)
    return jnp.sum(jnp.where(eye, row, 0.0), axis=1, keepdims=True)


def row_of(square):
    eye = iota((128, 128), 0) == iota((128, 128), 1)
    return jnp.sum(jnp.where(eye, square, 0.0), axis=0, keepdims=True)


def split3(value):
    high = value.astype(BF16)
    rest = value - high.astype(F32)
    mid = rest.astype(BF16)
    low = (rest - mid.astype(F32)).astype(BF16)
    return high, mid, low


def kernel(
    tokens,
    norm_gain,
    fox_query,
    fox_key,
    fox_value,
    cum_gate,
    lin_query,
    lin_key,
    lin_value,
    decay_down,
    decay_up,
    decay_bias,
    lin_gain,
    fox_out,
    lin_out,
    mixed,
    log_total,
    xg,
    w,
    wd,
    wo,
    acc,
    ssq,
    qs,
    kv,
    cq,
    top,
    oacc,
    ob,
    lb,
    op,
    lp,
    lcum,
    lout,
    qext,
    s1s,
    s1,
    s2,
    s3s,
    s3,
    heads,
    pb,
    pr,
    cb,
    raw,
    raws,
    fin,
    ss,
    rs,
    ls,
):
    z, x = lax.axis_index("z"), lax.axis_index("x")
    y, c = lax.axis_index("y"), lax.axis_index("c")
    other = 1 - c
    yp, ym, yo = lax.rem(y + 1, NY), lax.rem(y + 3, NY), lax.rem(y + 2, NY)
    zp, zm = lax.rem(z + 1, NZ), lax.rem(z + 7, NZ)
    sib = (z, x, y, other)
    up, down = (z, x, yp, c), (z, x, ym, c)
    z_up, z_down = (zp, x, y, c), (zm, x, y, c)

    sites = [0]
    pending = []

    def site():
        sites[0] += 1
        return sites[0] - 1

    def copy(src, dst, k, dev):
        return pltpu.make_async_remote_copy(
            src_ref=src,
            dst_ref=dst,
            send_sem=ss.at[k],
            recv_sem=rs.at[k],
            device_id=dev,
            device_id_type=MESH,
        )

    def send(src, dst, k, dev, when=None):
        if when is None:
            copy(src, dst, k, dev).start()
        else:
            pl.when(when)(lambda: copy(src, dst, k, dev).start())
        pending.append((src, dst, k, dev, when))

    def arrive(dst, k):
        copy(dst, dst, k, sib).wait_recv()

    own = y * 2 + c
    first = pltpu.make_async_copy(tokens, xg.at[own], ls.at[0])
    first.start()
    weights = []
    column = 0
    for n, ref in enumerate((fox_query, fox_key, fox_value, lin_query, lin_key, lin_value)):
        width = ref.shape[1]
        weights.append(pltpu.make_async_copy(ref, w.at[:, pl.ds(column, width)], ls.at[1 + n]))
        column += width
    weights.append(pltpu.make_async_copy(decay_down, wd, ls.at[7]))
    for item in weights:
        item.start()
    outs = [
        pltpu.make_async_copy(fox_out, wo.at[pl.ds(0, HEAD), :], ls.at[8]),
        pltpu.make_async_copy(lin_out, wo.at[pl.ds(HEAD, VAL), :], ls.at[9]),
    ]
    for item in outs:
        item.start()

    partners = [sib, up, down]
    partners += [(z, lax.rem(x + n, NX), y, c) for n in range(1, NX)]
    partners += [(lax.rem(z + n, NZ), x, y, c) for n in range(1, NZ)]
    barrier = pltpu.get_barrier_semaphore()
    for dev in partners:
        pl.semaphore_signal(barrier, inc=1, device_id=dev, device_id_type=MESH)
    pl.semaphore_wait(barrier, len(partners))

    first.wait()
    k_sib = site()
    k_up = [site() for _ in range(CHUNKS)]
    k_down = [site() for _ in range(CHUNKS)]
    k_far = [site() for _ in range(CHUNKS)]
    k_relay = [[site() for _ in range(CHUNKS)] for _ in range(3)]
    half = CHUNKS // 2

    def piece(block, n):
        return xg.at[block, pl.ds(n * ROWS, ROWS), :]

    def push(block, n, k, dev):
        send(piece(block, n), piece(block, n), k, dev)

    for n in range(CHUNKS):
        push(own, n, k_up[n], up)
        m = (n + half) % CHUNKS
        push(own, m, k_down[m], down)
    send(xg.at[own], xg.at[own], k_sib, sib)

    b_m, b_p, b_o = ym * 2 + c, yp * 2 + c, yo * 2 + c
    for item in weights:
        item.wait()
    w[:, pl.ds(896, 128)] = jnp.concatenate([wd[...], jnp.zeros((D, 112), BF16)], axis=1)
    acc[...] = jnp.zeros_like(acc)
    ssq[...] = jnp.zeros_like(ssq)

    def project(block):
        xb = xg[block].astype(F32)
        ssq[...] += jnp.sum(xb * xb, axis=1, keepdims=True)
        rows = pl.multiple_of(block * FEAT, FEAT)
        gain = norm_gain[:, pl.ds(rows, FEAT)]
        acc[...] += mm((xb * gain).astype(BF16), w[pl.ds(rows, FEAT), :])

    project(own)
    for n in range(half):
        m = n + half
        arrive(piece(b_m, n), k_up[n])
        push(b_m, n, k_far[n], up)
        push(b_m, n, k_relay[0][n], sib)
        arrive(piece(b_p, m), k_down[m])
        push(b_p, m, k_far[m], down)
        push(b_p, m, k_relay[1][m], sib)
    s_own, s_m, s_p, s_o = y * 2 + other, ym * 2 + other, yp * 2 + other, yo * 2 + other
    arrive(xg.at[s_own], k_sib)
    project(s_own)
    for n in range(half):
        m = n + half
        arrive(piece(b_m, m), k_up[m])
        push(b_m, m, k_relay[0][m], sib)
        arrive(piece(b_p, n), k_down[n])
        push(b_p, n, k_relay[1][n], sib)
    lax.fori_loop(0, 2, lambda i, _: project(jnp.where(i == 0, b_m, b_p)), None)
    for n in range(half):
        m = n + half
        arrive(piece(b_o, n), k_far[n])
        push(b_o, n, k_relay[2][n], sib)
        arrive(piece(b_o, m), k_far[m])
        push(b_o, m, k_relay[2][m], sib)
    for n in range(CHUNKS):
        arrive(piece(s_m, n), k_relay[0][n])
        arrive(piece(s_p, n), k_relay[1][n])

    def late(i, _):
        project(jnp.where(i == 0, s_m, jnp.where(i == 1, s_p, b_o)))

    lax.fori_loop(0, 3, late, None)
    for n in range(CHUNKS):
        arrive(piece(s_o, n), k_relay[2][n])
    project(s_o)

    norm = lax.rsqrt(ssq[:, 0:1] * (1.0 / D) + EPS)

    def result(start, width):
        return acc[:, pl.ds(start, width)] * norm

    qs[x] = (result(0, 128) * HEAD ** (-0.5)).astype(BF16)
    kv[z] = result(128, 256).astype(BF16)

    kv_half = KV_CHUNKS // 2

    def reach(n):
        return (4, 3) if n < kv_half else (3, 4)

    k_kv = {}
    for step in range(1, 5):
        for n in range(KV_CHUNKS):
            for way in (0, 1):
                if step <= reach(n)[way]:
                    k_kv[step, n, way] = site()

    def origin(step, way):
        return lax.rem(z + (NZ - step if way == 0 else step), NZ)

    def kv_piece(block, n):
        return kv.at[block, pl.ds(n * KV_ROWS, KV_ROWS), :]

    def kv_send(step, n, way):
        if (step, n, way) in k_kv:
            part = kv_piece(origin(step - 1, way), n)
            send(part, part, k_kv[step, n, way], z_down if way else z_up)

    def ring(step):
        for m in range(kv_half):
            for n, way in ((m, 0), (m + kv_half, 1)):
                arrive(kv_piece(origin(step, way), n), k_kv[step, n, way])
                kv_send(step + 1, n, way)
        for m in range(kv_half):
            for n, way in ((m + kv_half, 0), (m, 1)):
                if (step, n, way) in k_kv:
                    arrive(kv_piece(origin(step, way), n), k_kv[step, n, way])
                    kv_send(step + 1, n, way)

    for m in range(kv_half):
        kv_send(1, m, 0)
        kv_send(1, m + kv_half, 1)
    for m in range(kv_half):
        kv_send(1, m + kv_half, 0)
        kv_send(1, m, 1)

    def x_at(n):
        return lax.rem(x + n, NX)

    k_q = [site() for _ in range(NX)]
    for n in range(1, NX):
        send(qs.at[x], qs.at[x], k_q[n], (z, x_at(n), y, c))

    lk = result(512, 128).astype(BF16).astype(F32)
    lv = result(640, 256).astype(BF16)
    low = result(896, 128).astype(BF16)
    up_weight = jnp.concatenate([decay_up[...], jnp.zeros((112, 128), BF16)], axis=0)
    pre = mm(low, up_weight) + decay_bias[...]
    decay = (jnp.minimum(pre, 0.0) - jnp.log1p(jnp.exp(-jnp.abs(pre)))) * (1.0 / TAU)
    lower = (iota((TOK, TOK), 0) >= iota((TOK, TOK), 1)).astype(BF16)
    sums = mm(lower, jnp.concatenate(split3(decay), axis=1))
    cum = sums[:, 0:128] + sums[:, 128:256] + sums[:, 256:384]
    lcum[...] = cum
    last = cum[TOK - 1 : TOK, :]
    state = tn(lv, (lk * jnp.exp(last - cum)).astype(BF16))
    quarter = VAL // NX
    row16 = iota((16, 128), 0)

    def pack(ref, values, total):
        ref[pl.ds(0, quarter), :] = values.astype(BF16)
        parts = split3(total)
        tail = jnp.zeros((16, 128), F32)
        for n in range(3):
            tail = jnp.where(row16 == n, parts[n].astype(F32), tail)
        ref[pl.ds(quarter, 16), :] = tail.astype(BF16)

    def unpack(ref):
        values = ref[pl.ds(0, quarter), :].astype(F32)
        tail = ref[pl.ds(quarter, 16), :].astype(F32)
        total = tail[0:1, :] + tail[1:2, :] + tail[2:3, :]
        return values, total

    for n in range(NX):
        pack(s1s.at[n], state[n * quarter : (n + 1) * quarter, :], last)
    k_s1 = [site() for _ in range(NX)]
    for n in range(1, NX):
        send(s1s.at[x_at(n)], s1.at[x], k_s1[n], (z, x_at(n), y, c))

    ring(1)

    lq = result(384, 128).astype(BF16).astype(F32) * KEY_SCALE
    qext[...] = (lq * jnp.exp(cum)).astype(BF16)
    rows_i, cols_j = iota((TOK, TOK), 0), iota((TOK, TOK), 1)
    row_id = iota((TOK, HEAD), 0)
    grouped = (TOK // 8, 8, HEAD)
    q8, k8, c8 = lq.reshape(grouped), lk.reshape(grouped), cum.reshape(grouped)
    place = iota(grouped, 1)
    total = jnp.zeros((TOK, TOK), F32)
    for back in range(8):
        if back:
            gap = jnp.where(place >= back, c8 - pltpu.roll(c8, back, 1), -jnp.inf)
            product = q8 * pltpu.roll(k8, back, 1) * jnp.exp(gap)
        else:
            product = q8 * k8
        one = jnp.sum(product.reshape(TOK, HEAD), axis=1, keepdims=True)
        total = jnp.where(rows_i - cols_j == back, one, total)
    span = 8
    while span < TOK:
        pairs = (TOK // (2 * span), 2 * span, HEAD)
        edge = jnp.broadcast_to(cum.reshape(pairs)[:, span - 1 : span, :], pairs).reshape(TOK, HEAD)
        right = (row_id // span) % 2 == 1
        fall = jnp.exp(-jnp.abs(cum - edge))
        q_part = jnp.where(right, lq * fall, 0.0).astype(BF16)
        k_part = jnp.where(right, 0.0, lk * fall).astype(BF16)
        same = rows_i // (2 * span) == cols_j // (2 * span)
        total = total + jnp.where(same, nt(q_part, k_part), 0.0)
        span *= 2
    lout[...] = mm(total.astype(BF16), lv)

    for n in range(1, NX):
        arrive(qs.at[x_at(NX - n)], k_q[n])
    for j in range(NX):
        for n in range(2):
            start = pl.multiple_of((z * NX + j) * TOK + n * 128, 128)
            column_gate = column_of(cum_gate[:, pl.ds(start, 128)])
            cq[j, pl.ds(n * 128, 128), :] = jnp.broadcast_to(column_gate, (128, 128))

    def logits(j, block):
        start = pl.multiple_of((block * NX + x) * TOK, TOK)
        gate = cum_gate[:, pl.ds(start, TOK)]
        return nt(qs[j], kv[block, :, pl.ds(0, HEAD)]) + (cq[j][:, 0:1] - gate)

    def values(block):
        return jnp.concatenate(
            [kv[block, :, pl.ds(HEAD, HEAD)], jnp.ones((TOK, HEAD), BF16)], axis=1
        )

    def diagonal(j, _):
        seen = iota((TOK, TOK), 1) + x * TOK <= iota((TOK, TOK), 0) + j * TOK
        logit = jnp.where(seen, logits(j, z), LOW)
        peak = jnp.max(logit, axis=1, keepdims=True)
        top[j] = jnp.broadcast_to(peak, (TOK, HEAD))
        oacc[j] = mm(jnp.exp(logit - peak).astype(BF16), values(z))

    lax.fori_loop(0, NX, diagonal, None)

    def attend(block):
        def one(j, _):
            logit = logits(j, block)
            old = top[j][:, 0:1]
            peak = jnp.maximum(old, jnp.max(logit, axis=1, keepdims=True))
            top[j] = jnp.broadcast_to(peak, (TOK, HEAD))
            weight = jnp.exp(logit - peak).astype(BF16)
            oacc[j] = oacc[j] * jnp.exp(old - peak) + mm(weight, values(block))

        pl.when(block < z)(lambda: lax.fori_loop(0, NX, one, None))

    def attend_both(step):
        def one(way, _):
            attend(lax.rem(z + jnp.where(way == 0, NZ - step, step), NZ))

        lax.fori_loop(0, 2, one, None)

    ring(2)
    attend_both(1)

    for n in range(1, NX):
        arrive(s1.at[x_at(NX - n)], k_s1[n])
    s1[x] = s1s[x]
    row_state, row_total = jnp.zeros((quarter, 128), F32), jnp.zeros((1, 128), F32)
    for n in range(NX):
        values_n, total_n = unpack(s1.at[n])
        row_state = jnp.exp(total_n) * row_state + values_n
        row_total = row_total + total_n
    pack(s2.at[z], row_state, row_total)
    k_s2 = [site() for _ in range(NZ)]
    for n in range(1, NZ):
        send(s2.at[z], s2.at[z], k_s2[n], (lax.rem(z + n, NZ), x, y, c), when=z + n < NZ)

    ring(3)
    attend_both(2)

    for n in range(1, NZ):
        before = lax.rem(z + NZ - n, NZ)
        pl.when(z >= n)(lambda before=before, n=n: arrive(s2.at[before], k_s2[n]))

    def earlier(n, state):
        values_n, total_n = unpack(s2.at[n])
        return jnp.exp(total_n) * state + values_n

    state = lax.fori_loop(0, z, earlier, jnp.zeros((quarter, 128), F32))
    for n in range(NX):
        s3s[n] = state.astype(BF16)
        values_n, total_n = unpack(s1.at[n])
        state = jnp.exp(total_n) * state + values_n
    k_s3 = [site() for _ in range(NX)]
    for n in range(1, NX):
        send(s3s.at[x_at(n)], s3.at[x], k_s3[n], (z, x_at(n), y, c))

    ring(4)
    attend_both(3)
    attend(lax.rem(z + 4, NZ))

    def close(j, _):
        mass = oacc[j][:, HEAD:]
        op[j] = (oacc[j][:, 0:HEAD] / mass).astype(BF16)
        height = top[j] + jnp.log(mass)
        first_row, second_row = row_of(height[0:128]), row_of(height[128:256])
        row8 = iota((8, 128), 0)
        lp[j] = jnp.where(row8 == 0, first_row, jnp.where(row8 == 1, second_row, 0.0))

    lax.fori_loop(0, NX, close, None)
    k_o = [site() for _ in range(NX)]
    k_l = [site() for _ in range(NX)]
    for n in range(1, NX):
        dev = (z, x_at(n), y, c)
        send(op.at[x_at(n)], ob.at[x], k_o[n], dev)
        send(lp.at[x_at(n)], lb.at[x], k_l[n], dev)

    for n in range(1, NX):
        arrive(s3.at[x_at(NX - n)], k_s3[n])
    s3[x] = s3s[x]
    whole = jnp.concatenate([s3[n] for n in range(NX)], axis=0)
    lin_raw = lout[...] + nt(qext[...], whole)
    mean = jnp.mean(lin_raw * lin_raw, axis=1, keepdims=True)
    heads[:, pl.ds(HEAD, VAL)] = (lin_raw * lax.rsqrt(mean + EPS) * lin_gain[...]).astype(BF16)

    for n in range(1, NX):
        arrive(ob.at[x_at(NX - n)], k_o[n])
        arrive(lb.at[x_at(NX - n)], k_l[n])
    ob[x] = op[x]
    lb[x] = lp[x]
    heights = [lb[n] for n in range(NX)]
    peak = jnp.maximum(jnp.maximum(heights[0], heights[1]), jnp.maximum(heights[2], heights[3]))
    shares = [jnp.exp(h - peak) for h in heights]
    mass = shares[0] + shares[1] + shares[2] + shares[3]
    summit = peak + jnp.log(mass)
    for n in range(2):
        rows = pl.ds(n * 128, 128)
        log_total[:, rows] = summit[n : n + 1, :]
        mix = jnp.zeros((128, HEAD), F32)
        for m in range(NX):
            share = column_of((shares[m] / mass)[n : n + 1, :])
            mix = mix + share * ob[m, rows, :].astype(F32)
        heads[rows, pl.ds(0, HEAD)] = mix.astype(BF16)

    for item in outs:
        item.wait()
    k_pair = [site() for _ in range(COL_CHUNKS)]
    k_raw = [site() for _ in range(COL_CHUNKS)]
    k_fin = [[site() for _ in range(2)] for _ in range(COL_CHUNKS)]
    col_half = COL_CHUNKS // 2
    order = [n + half_n for n in range(col_half) for half_n in (0, col_half)]

    def produce(n):
        part = mm(heads[...], wo[:, pl.ds(n * COLS, COLS)]).astype(BF16)
        part = part.reshape(NY, NC, 32, COLS)
        for m in range(NC):
            pb[n, m] = part[:, m]
        send(pb.at[n, other], pr.at[n], k_pair[n], sib)

    def spread(n):
        arrive(pr.at[n], k_pair[n])
        cb[n] = (pb[n, c].astype(F32) + pr[n].astype(F32)).astype(BF16)
        near, far = (down, up) if n < col_half else (up, down)
        y_near = ym if n < col_half else yp
        send(cb.at[n, yo], raw.at[n], k_raw[n], far)
        send(cb.at[n, y_near], fin.at[n, 1], k_fin[n][1], near)

    def relay(n):
        arrive(raw.at[n], k_raw[n])
        far, y_far = (up, yp) if n < col_half else (down, ym)
        raws[n] = (cb[n, y_far].astype(F32) + raw[n].astype(F32)).astype(BF16)
        send(raws.at[n], fin.at[n, 0], k_fin[n][0], far)

    def finish(n):
        for m in range(2):
            arrive(fin.at[n, m], k_fin[n][m])
        done = cb[n, y].astype(F32) + fin[n, 0].astype(F32) + fin[n, 1].astype(F32)
        mixed[:, pl.ds(n * COLS, COLS)] = done.astype(BF16)

    for i in range(COL_CHUNKS + 1):
        if i < COL_CHUNKS:
            produce(order[i])
        if i:
            spread(order[i - 1])
    for n in order:
        relay(n)
    for n in order:
        finish(n)

    for src, dst, k, dev, when in pending:
        if when is None:
            copy(src, dst, k, dev).wait_send()
        else:
            pl.when(when)(lambda a=(src, dst, k, dev): copy(*a).wait_send())


def vmem(shape, dtype):
    return pltpu.VMEM(shape, dtype)


SCRATCH = [
    vmem((NY * NC, TOK, FEAT), BF16),
    vmem((D, 1024), BF16),
    vmem((D, 16), BF16),
    vmem((HEAD + VAL, D), BF16),
    vmem((TOK, 1024), F32),
    vmem((TOK, 128), F32),
    vmem((NX, TOK, HEAD), BF16),
    vmem((NZ, TOK, 2 * HEAD), BF16),
    vmem((NX, TOK, 128), F32),
    vmem((NX, TOK, 128), F32),
    vmem((NX, TOK, 2 * HEAD), F32),
    vmem((NX, TOK, HEAD), BF16),
    vmem((NX, 8, 128), F32),
    vmem((NX, TOK, HEAD), BF16),
    vmem((NX, 8, 128), F32),
    vmem((TOK, 128), F32),
    vmem((TOK, VAL), F32),
    vmem((TOK, 128), BF16),
    vmem((NX, VAL // NX + 16, 128), BF16),
    vmem((NX, VAL // NX + 16, 128), BF16),
    vmem((NZ, VAL // NX + 16, 128), BF16),
    vmem((NX, VAL // NX, 128), BF16),
    vmem((NX, VAL // NX, 128), BF16),
    vmem((TOK, HEAD + VAL), BF16),
    vmem((COL_CHUNKS, NC, NY, 32, COLS), BF16),
    vmem((COL_CHUNKS, NY, 32, COLS), BF16),
    vmem((COL_CHUNKS, NY, 32, COLS), BF16),
    vmem((COL_CHUNKS, 32, COLS), BF16),
    vmem((COL_CHUNKS, 32, COLS), BF16),
    vmem((COL_CHUNKS, 2, 32, COLS), BF16),
    pltpu.SemaphoreType.DMA((N_SEM,)),
    pltpu.SemaphoreType.DMA((N_SEM,)),
    pltpu.SemaphoreType.DMA((N_LOC,)),
]


def local(
    tokens,
    norm_gain,
    fox_query,
    fox_key,
    fox_value,
    cum_gate,
    lin_query,
    lin_key,
    lin_value,
    decay_down,
    decay_up,
    decay_bias,
    lin_gain,
    fox_out,
    lin_out,
):
    here = pl.BlockSpec(memory_space=pltpu.VMEM)
    far = pl.BlockSpec(memory_space=pl.ANY)
    specs = [far, here, far, far, far, here, far, far, far, far, here, here, here, far, far]
    return pl.pallas_call(
        kernel,
        name="layer",
        out_shape=(
            jax.ShapeDtypeStruct((32, D), BF16),
            jax.ShapeDtypeStruct((1, TOK), F32),
        ),
        in_specs=specs,
        out_specs=(here, here),
        scratch_shapes=SCRATCH,
        compiler_params=pltpu.CompilerParams(
            collective_id=0, has_side_effects=True, vmem_limit_bytes=60 * 1024 * 1024
        ),
    )(
        tokens,
        norm_gain.reshape(1, D),
        fox_query,
        fox_key,
        fox_value,
        cum_gate,
        lin_query,
        lin_key,
        lin_value,
        decay_down,
        decay_up,
        decay_bias.reshape(1, HEAD),
        lin_gain.reshape(1, VAL),
        fox_out,
        lin_out,
    )


def solution(mesh):
    torus = Mesh(mesh.devices.reshape(NZ, NX, NY, NC), ("z", "x", "y", "c"))
    sp, tp, sp_tp = ("z", "x"), ("y", "c"), ("z", "x", "y", "c")
    in_specs = (
        P(sp, tp),
        P(),
        P(None, tp),
        P(None, tp),
        P(None, tp),
        P(tp, None),
        P(None, tp),
        P(None, tp),
        P(None, tp),
        P(),
        P(None, tp),
        P(tp),
        P(),
        P(tp, None),
        P(tp, None),
    )
    out_specs = (P(sp_tp, None), P(tp, sp))
    return jax.shard_map(local, mesh=torus, in_specs=in_specs, out_specs=out_specs, check_vma=False)
```

```python
import jax
import jax.numpy as jnp
from jax import lax
from jax.experimental import pallas as pl
from jax.experimental.pallas import tpu as pltpu
from jax.sharding import Mesh
from jax.sharding import PartitionSpec as P

MESH = pl.DeviceIdType.MESH
F32 = jnp.float32
BF16 = jnp.bfloat16

NZ, NX, NY, NC = 8, 4, 4, 2
TOK = 256
D = 4096
FEAT = 512
HEAD = 128
VAL = 256
EPS = 1e-06
TAU = 16.0
LOW = -3.0e38
KEY_SCALE = 128 ** (-0.5)

CHUNKS = 4
ROWS = TOK // CHUNKS
KV_CHUNKS = 4
KV_ROWS = TOK // KV_CHUNKS
COL_CHUNKS = 8
COLS = D // COL_CHUNKS
N_SEM = 160
N_LOC = 16


def nt(a, b):
    return lax.dot_general(a, b, (((1,), (1,)), ((), ())), preferred_element_type=F32)


def tn(a, b):
    return lax.dot_general(a, b, (((0,), (0,)), ((), ())), preferred_element_type=F32)


def mm(a, b):
    return jnp.dot(a, b, preferred_element_type=F32)


def iota(shape, dim):
    return lax.broadcasted_iota(jnp.int32, shape, dim)


def column_of(row):
    eye = iota((128, 128), 0) == iota((128, 128), 1)
    return jnp.sum(jnp.where(eye, row, 0.0), axis=1, keepdims=True)


def row_of(square):
    eye = iota((128, 128), 0) == iota((128, 128), 1)
    return jnp.sum(jnp.where(eye, square, 0.0), axis=0, keepdims=True)


def split3(value):
    high = value.astype(BF16)
    rest = value - high.astype(F32)
    mid = rest.astype(BF16)
    low = (rest - mid.astype(F32)).astype(BF16)
    return high, mid, low


def kernel(
    tokens,
    norm_gain_far,
    fox_query,
    fox_key,
    fox_value,
    cum_gate_far,
    lin_query,
    lin_key,
    lin_value,
    decay_down,
    decay_up_far,
    decay_bias_far,
    lin_gain_far,
    fox_out,
    lin_out,
    own_part,
    fin,
    log_total,
    xg,
    w,
    wd,
    wo,
    acc,
    ssq,
    qs,
    kv,
    cq,
    top,
    oacc,
    ob,
    lb,
    op,
    lp,
    share,
    lcum,
    lout,
    qext,
    s1s,
    s1,
    s2,
    s3s,
    s3,
    heads,
    pb,
    pr,
    cb,
    raw,
    raws,
    norm_gain,
    cum_gate,
    decay_up,
    decay_bias,
    lin_gain,
    ss,
    rs,
    ls,
):
    z, x = lax.axis_index("z"), lax.axis_index("x")
    y, c = lax.axis_index("y"), lax.axis_index("c")
    other = 1 - c
    yp, ym, yo = lax.rem(y + 1, NY), lax.rem(y + 3, NY), lax.rem(y + 2, NY)
    zp, zm = lax.rem(z + 1, NZ), lax.rem(z + 7, NZ)
    sib = (z, x, y, other)
    up, down = (z, x, yp, c), (z, x, ym, c)
    z_up, z_down = (zp, x, y, c), (zm, x, y, c)

    sites = [0]
    pending = []

    def site():
        sites[0] += 1
        return sites[0] - 1

    def copy(src, dst, k, dev):
        return pltpu.make_async_remote_copy(
            src_ref=src,
            dst_ref=dst,
            send_sem=ss.at[k],
            recv_sem=rs.at[k],
            device_id=dev,
            device_id_type=MESH,
        )

    def send(src, dst, k, dev, when=None):
        if when is None:
            copy(src, dst, k, dev).start()
        else:
            pl.when(when)(lambda: copy(src, dst, k, dev).start())
        pending.append((src, dst, k, dev, when))

    def arrive(dst, k):
        copy(dst, dst, k, sib).wait_recv()

    own = y * 2 + c
    first = pltpu.make_async_copy(tokens, xg.at[own], ls.at[0])
    first.start()
    weights = []
    column = 0
    for n, ref in enumerate((fox_query, fox_key, fox_value, lin_query, lin_key, lin_value)):
        width = ref.shape[1]
        weights.append(pltpu.make_async_copy(ref, w.at[:, pl.ds(column, width)], ls.at[1 + n]))
        column += width
    weights.append(pltpu.make_async_copy(decay_down, wd, ls.at[7]))
    smalls = [
        pltpu.make_async_copy(norm_gain_far, norm_gain, ls.at[10]),
        pltpu.make_async_copy(cum_gate_far, cum_gate, ls.at[11]),
        pltpu.make_async_copy(decay_up_far, decay_up, ls.at[12]),
        pltpu.make_async_copy(decay_bias_far, decay_bias, ls.at[13]),
        pltpu.make_async_copy(lin_gain_far, lin_gain, ls.at[14]),
    ]
    weights = smalls + weights
    for item in weights:
        item.start()
    outs = [
        pltpu.make_async_copy(fox_out, wo.at[pl.ds(0, HEAD), :], ls.at[8]),
        pltpu.make_async_copy(lin_out, wo.at[pl.ds(HEAD, VAL), :], ls.at[9]),
    ]
    for item in outs:
        item.start()

    partners = [sib, up, down]
    partners += [(z, lax.rem(x + n, NX), y, c) for n in range(1, NX)]
    z_four = (lax.rem(z + 4, NZ), x, y, c)
    partners += [z_up, z_down, z_four]
    barrier = pltpu.get_barrier_semaphore()
    for dev in partners:
        pl.semaphore_signal(barrier, inc=1, device_id=dev, device_id_type=MESH)
    pl.semaphore_wait(barrier, len(partners))

    first.wait()
    k_sib = site()
    k_up = [site() for _ in range(CHUNKS)]
    k_down = [site() for _ in range(CHUNKS)]
    k_far = [site() for _ in range(CHUNKS)]
    k_relay = [[site() for _ in range(CHUNKS)] for _ in range(3)]
    half = CHUNKS // 2

    def piece(block, n):
        return xg.at[block, pl.ds(n * ROWS, ROWS), :]

    def push(block, n, k, dev):
        send(piece(block, n), piece(block, n), k, dev)

    for n in range(CHUNKS):
        push(own, n, k_up[n], up)
        m = (n + half) % CHUNKS
        push(own, m, k_down[m], down)
    send(xg.at[own], xg.at[own], k_sib, sib)

    b_m, b_p, b_o = ym * 2 + c, yp * 2 + c, yo * 2 + c
    for item in weights:
        item.wait()

    def widen(i, _):
        rows = pl.ds(pl.multiple_of(i * FEAT, FEAT), FEAT)
        part = jnp.concatenate([wd[:, rows].astype(F32), jnp.zeros((112, FEAT), F32)], axis=0)
        w[rows, pl.ds(896, 128)] = part.T.astype(BF16)

    lax.fori_loop(0, NY * NC, widen, None)
    acc[...] = jnp.zeros_like(acc)
    ssq[...] = jnp.zeros_like(ssq)

    def project(block):
        xb = xg[block].astype(F32)
        ssq[...] += jnp.sum(xb * xb, axis=1, keepdims=True)
        rows = pl.multiple_of(block * FEAT, FEAT)
        gain = norm_gain[:, pl.ds(rows, FEAT)]
        acc[...] += mm((xb * gain).astype(BF16), w[pl.ds(rows, FEAT), :])

    project(own)
    for n in range(half):
        m = n + half
        arrive(piece(b_m, n), k_up[n])
        push(b_m, n, k_far[n], up)
        push(b_m, n, k_relay[0][n], sib)
        arrive(piece(b_p, m), k_down[m])
        push(b_p, m, k_far[m], down)
        push(b_p, m, k_relay[1][m], sib)
    s_own, s_m, s_p, s_o = y * 2 + other, ym * 2 + other, yp * 2 + other, yo * 2 + other
    arrive(xg.at[s_own], k_sib)
    project(s_own)
    for n in range(half):
        m = n + half
        arrive(piece(b_m, m), k_up[m])
        push(b_m, m, k_relay[0][m], sib)
        arrive(piece(b_p, n), k_down[n])
        push(b_p, n, k_relay[1][n], sib)
    project(b_m)
    project(b_p)
    late_blocks = (s_m, s_p)
    for n in range(half):
        m = n + half
        arrive(piece(b_o, n), k_far[n])
        push(b_o, n, k_relay[2][n], sib)
        arrive(piece(b_o, m), k_far[m])
        push(b_o, m, k_relay[2][m], sib)
        if n < 2:
            for r in range(CHUNKS):
                arrive(piece(late_blocks[n], r), k_relay[n][r])
            project(late_blocks[n])
    project(b_o)
    for n in range(CHUNKS):
        arrive(piece(s_o, n), k_relay[2][n])
    project(s_o)

    norm = lax.rsqrt(ssq[:, 0:1] * (1.0 / D) + EPS)

    def result(start, width):
        return acc[:, pl.ds(start, width)] * norm

    qs[x] = (result(0, 128) * HEAD ** (-0.5)).astype(BF16)
    kv[z] = result(128, 256).astype(BF16)

    kv_half = KV_CHUNKS // 2

    def reach(n):
        return (4, 3) if n < kv_half else (3, 4)

    k_kv = {}
    for step in range(1, 5):
        for n in range(KV_CHUNKS):
            for way in (0, 1):
                if step <= reach(n)[way]:
                    k_kv[step, n, way] = site()

    def origin(step, way):
        return lax.rem(z + (NZ - step if way == 0 else step), NZ)

    def kv_piece(block, n):
        return kv.at[block, pl.ds(n * KV_ROWS, KV_ROWS), :]

    def wanted(step, n, way, receiver):
        if way == 0:
            return receiver >= step
        far = receiver + step
        return jnp.logical_or(far >= NZ, far + 1 <= reach(n)[1])

    def kv_send(step, n, way):
        if (step, n, way) in k_kv:
            part = kv_piece(origin(step - 1, way), n)
            dev, receiver = (z_down, zm) if way else (z_up, zp)
            send(part, part, k_kv[step, n, way], dev, wanted(step, n, way, receiver))

    def kv_step(step, n, way):
        if (step, n, way) in k_kv:
            part = kv_piece(origin(step, way), n)
            k = k_kv[step, n, way]
            pl.when(wanted(step, n, way, z))(lambda: arrive(part, k))
            kv_send(step + 1, n, way)

    def slot(step, number):
        m = number % kv_half
        pairs = ((m, 0), (m + kv_half, 1)) if number < kv_half else ((m + kv_half, 0), (m, 1))
        for n, way in pairs:
            kv_step(step, n, way)

    for m in range(kv_half):
        kv_send(1, m, 0)
        kv_send(1, m + kv_half, 1)
    for m in range(kv_half):
        kv_send(1, m + kv_half, 0)
        kv_send(1, m, 1)

    def x_at(n):
        return lax.rem(x + n, NX)

    lk = result(512, 128).astype(BF16).astype(F32)
    lv = result(640, 256).astype(BF16)
    low = result(896, 128).astype(BF16)
    up_weight = jnp.concatenate([decay_up[...], jnp.zeros((112, 128), BF16)], axis=0)
    pre = mm(low, up_weight) + decay_bias[...]
    decay = (jnp.minimum(pre, 0.0) - jnp.log1p(jnp.exp(-jnp.abs(pre)))) * (1.0 / TAU)
    lower = (iota((TOK, TOK), 0) >= iota((TOK, TOK), 1)).astype(BF16)
    sums = mm(lower, jnp.concatenate(split3(decay), axis=1))
    cum = sums[:, 0:128] + sums[:, 128:256] + sums[:, 256:384]
    lcum[...] = cum
    last = cum[TOK - 1 : TOK, :]
    state = tn(lv, (lk * jnp.exp(last - cum)).astype(BF16))
    quarter = VAL // NX
    row16 = iota((16, 128), 0)

    def pack(ref, values, total):
        ref[pl.ds(0, quarter), :] = values.astype(BF16)
        parts = split3(total)
        tail = jnp.zeros((16, 128), F32)
        for n in range(3):
            tail = jnp.where(row16 == n, parts[n].astype(F32), tail)
        ref[pl.ds(quarter, 16), :] = tail.astype(BF16)

    def unpack(ref):
        values = ref[pl.ds(0, quarter), :].astype(F32)
        tail = ref[pl.ds(quarter, 16), :].astype(F32)
        total = tail[0:1, :] + tail[1:2, :] + tail[2:3, :]
        return values, total

    for n in range(NX):
        pack(s1s.at[n], state[n * quarter : (n + 1) * quarter, :], last)
    k_s1 = [site() for _ in range(NX)]
    for n in range(1, NX):
        send(s1s.at[x_at(n)], s1.at[x], k_s1[n], (z, x_at(n), y, c))

    k_q = [site() for _ in range(NX)]
    for n in range(1, NX):
        send(qs.at[x], qs.at[x], k_q[n], (z, x_at(n), y, c))

    lq = result(384, 128).astype(BF16).astype(F32) * KEY_SCALE
    qext[...] = (lq * jnp.exp(cum)).astype(BF16)
    rows_i, cols_j = iota((TOK, TOK), 0), iota((TOK, TOK), 1)
    row_id = iota((TOK, HEAD), 0)
    grouped = (TOK // 8, 8, HEAD)
    q8, k8, c8 = lq.reshape(grouped), lk.reshape(grouped), cum.reshape(grouped)
    place = iota(grouped, 1)
    total = jnp.zeros((TOK, TOK), F32)
    for back in range(8):
        if back:
            gap = jnp.where(place >= back, c8 - pltpu.roll(c8, back, 1), -jnp.inf)
            product = q8 * pltpu.roll(k8, back, 1) * jnp.exp(gap)
        else:
            product = q8 * k8
        one = jnp.sum(product.reshape(TOK, HEAD), axis=1, keepdims=True)
        total = jnp.where(rows_i - cols_j == back, one, total)
    span = 8
    while span < TOK:
        pairs = (TOK // (2 * span), 2 * span, HEAD)
        edge = jnp.broadcast_to(cum.reshape(pairs)[:, span - 1 : span, :], pairs).reshape(TOK, HEAD)
        right = (row_id // span) % 2 == 1
        fall = jnp.exp(-jnp.abs(cum - edge))
        q_part = jnp.where(right, lq * fall, 0.0).astype(BF16)
        k_part = jnp.where(right, 0.0, lk * fall).astype(BF16)
        same = rows_i // (2 * span) == cols_j // (2 * span)
        total = total + jnp.where(same, nt(q_part, k_part), 0.0)
        span *= 2
    lout[...] = mm(total.astype(BF16), lv)

    for j in range(NX):
        for n in range(2):
            start = pl.multiple_of((z * NX + j) * TOK + n * 128, 128)
            column_gate = column_of(cum_gate[:, pl.ds(start, 128)])
            cq[j, pl.ds(n * 128, 128), :] = jnp.broadcast_to(column_gate, (128, 128))

    def logits(j, block):
        start = pl.multiple_of((block * NX + x) * TOK, TOK)
        gate = cum_gate[:, pl.ds(start, TOK)]
        own_gate = cq[j]
        own_gate = jnp.concatenate([own_gate, own_gate], axis=1)
        return nt(qs[j], kv[block, :, pl.ds(0, HEAD)]) + (own_gate - gate)

    def values(block):
        return jnp.concatenate(
            [kv[block, :, pl.ds(HEAD, HEAD)], jnp.ones((TOK, HEAD), BF16)], axis=1
        )

    def diagonal(some):
        mine = values(z)
        for j in some:
            seen = iota((TOK, TOK), 1) + x * TOK <= iota((TOK, TOK), 0) + j * TOK
            logit = jnp.where(seen, logits(j, z), LOW)
            peak = jnp.max(logit, axis=1, keepdims=True)
            top[j] = jnp.broadcast_to(peak, (TOK, HEAD))
            oacc[j] = mm(jnp.exp(logit - peak).astype(BF16), mine)

    def update(block, some):
        theirs = values(block)
        for j in some:
            logit = logits(j, block)
            old = top[j]
            peak = jnp.maximum(old, jnp.max(logit, axis=1, keepdims=True))
            top[j] = peak
            wide = jnp.concatenate([peak, peak], axis=1)
            weight = jnp.exp(logit - wide).astype(BF16)
            fade = jnp.exp(old - peak)
            fade = jnp.concatenate([fade, fade], axis=1)
            oacc[j] = oacc[j] * fade + mm(weight, theirs)

    def attend(step, way):
        block = origin(step, way)
        pl.when(block < z)(lambda: update(block, range(NX)))

    slot(1, 0)
    slot(1, 1)
    slot(1, 2)
    slot(1, 3)

    for n in range(1, NX):
        arrive(s1.at[x_at(NX - n)], k_s1[n])
    s1[x] = s1s[x]
    row_state, row_total = jnp.zeros((quarter, 128), F32), jnp.zeros((1, 128), F32)
    for n in range(NX):
        values_n, total_n = unpack(s1.at[n])
        row_state = jnp.exp(total_n) * row_state + values_n
        row_total = row_total + total_n
    pack(s2.at[z], row_state, row_total)
    k_s2 = {(step, way): site() for step in range(1, 4) for way in (0, 1)}
    k_far_state = site()

    def state_send(step, way):
        if (step, way) in k_s2:
            dev, receiver = (z_down, zm) if way else (z_up, zp)
            part = s2.at[origin(step - 1, way)]
            send(part, part, k_s2[step, way], dev, wanted(step, 0, way, receiver))

    def state_step(step):
        for way in (0, 1):
            if (step, way) in k_s2:
                part, k = s2.at[origin(step, way)], k_s2[step, way]
                pl.when(wanted(step, 0, way, z))(lambda part=part, k=k: arrive(part, k))
                state_send(step + 1, way)

    state_send(1, 0)
    state_send(1, 1)
    send(s2.at[z], s2.at[z], k_far_state, z_four, z < 4)

    diagonal([x])
    slot(2, 0)
    slot(2, 1)
    for n in range(1, NX):
        arrive(qs.at[x_at(NX - n)], k_q[n])
    diagonal([x_at(n) for n in range(1, NX)])
    slot(2, 2)
    attend(1, 0)
    slot(2, 3)
    attend(1, 1)
    state_step(1)
    slot(3, 0)
    slot(3, 1)
    attend(2, 0)
    slot(3, 2)
    slot(3, 3)
    attend(2, 1)
    state_step(2)
    attend(3, 0)
    slot(4, 0)
    attend(3, 1)
    slot(4, 1)

    k_o = [site() for _ in range(NX)]
    k_l = [site() for _ in range(NX)]
    row8 = iota((8, 128), 0)
    for pair in ((2, 1), (3, 0)):
        some = [x_at(n) for n in pair]
        pl.when(z >= 4)(lambda some=some: update(origin(4, 0), some))
        for n, j in zip(pair, some):
            mass = oacc[j][:, HEAD:]
            op[j] = (oacc[j][:, 0:HEAD] / mass).astype(BF16)
            if n:
                send(op.at[j], ob.at[x], k_o[n], (z, j, y, c))
            height = top[j] + jnp.log(mass)
            first_row, second_row = row_of(height[0:128]), row_of(height[128:256])
            lp[j] = jnp.where(row8 == 0, first_row, jnp.where(row8 == 1, second_row, 0.0))
            if n:
                send(lp.at[j], lb.at[x], k_l[n], (z, j, y, c))

    state_step(3)
    far_state = s2.at[lax.rem(z + 4, NZ)]
    pl.when(z >= 4)(lambda: arrive(far_state, k_far_state))

    def earlier(n, state):
        values_n, total_n = unpack(s2.at[n])
        return jnp.exp(total_n) * state + values_n

    state = lax.fori_loop(0, z, earlier, jnp.zeros((quarter, 128), F32))
    for n in range(NX):
        s3s[n] = state.astype(BF16)
        values_n, total_n = unpack(s1.at[n])
        state = jnp.exp(total_n) * state + values_n
    k_s3 = [site() for _ in range(NX)]
    for n in range(1, NX):
        send(s3s.at[x_at(n)], s3.at[x], k_s3[n], (z, x_at(n), y, c))
    for n in range(1, NX):
        arrive(s3.at[x_at(NX - n)], k_s3[n])
    s3[x] = s3s[x]
    whole = jnp.concatenate([s3[n] for n in range(NX)], axis=0)
    lin_raw = lout[...] + nt(qext[...], whole)
    mean = jnp.mean(lin_raw * lin_raw, axis=1, keepdims=True)
    heads[:, pl.ds(HEAD, VAL)] = (lin_raw * lax.rsqrt(mean + EPS) * lin_gain[...]).astype(BF16)

    for n in range(1, NX):
        arrive(lb.at[x_at(NX - n)], k_l[n])
    lb[x] = lp[x]
    ob[x] = op[x]
    heights = [lb[n] for n in range(NX)]
    peak = jnp.maximum(jnp.maximum(heights[0], heights[1]), jnp.maximum(heights[2], heights[3]))
    shares = [jnp.exp(h - peak) for h in heights]
    mass = shares[0] + shares[1] + shares[2] + shares[3]
    summit = peak + jnp.log(mass)
    for n in range(2):
        rows = pl.ds(n * 128, 128)
        log_total[:, rows] = summit[n : n + 1, :]
        for m in range(NX):
            share[m, rows, :] = jnp.broadcast_to(
                column_of((shares[m] / mass)[n : n + 1, :]), (128, HEAD)
            )
    for n in range(1, NX):
        arrive(ob.at[x_at(NX - n)], k_o[n])
    mix = share[0] * ob[0].astype(F32)
    for m in range(1, NX):
        mix = mix + share[m] * ob[m].astype(F32)
    heads[:, pl.ds(0, HEAD)] = mix.astype(BF16)

    for item in outs:
        item.wait()
    def landing(n, m):
        return fin.at[m, :, pl.ds(n * COLS, COLS)]

    k_pair = [site() for _ in range(COL_CHUNKS)]
    k_raw = [site() for _ in range(COL_CHUNKS)]
    k_fin = [[site() for _ in range(2)] for _ in range(COL_CHUNKS)]
    col_half = COL_CHUNKS // 2
    order = [n + half_n for n in range(col_half) for half_n in (0, col_half)]

    def produce(n):
        part = mm(heads[...], wo[:, pl.ds(n * COLS, COLS)]).astype(BF16)
        part = part.reshape(NY, NC, 32, COLS)
        for m in range(NC):
            pb[n, m] = part[:, m]
        send(pb.at[n, other], pr.at[n], k_pair[n], sib)

    def spread(n):
        arrive(pr.at[n], k_pair[n])
        cb[n] = (pb[n, c].astype(F32) + pr[n].astype(F32)).astype(BF16)
        own_part[:, pl.ds(n * COLS, COLS)] = cb[n, y]
        near, far = (down, up) if n < col_half else (up, down)
        y_near = ym if n < col_half else yp
        send(cb.at[n, yo], raw.at[n], k_raw[n], far)
        send(cb.at[n, y_near], landing(n, 1), k_fin[n][1], near)

    def relay(n):
        arrive(raw.at[n], k_raw[n])
        far, y_far = (up, yp) if n < col_half else (down, ym)
        raws[n] = (cb[n, y_far].astype(F32) + raw[n].astype(F32)).astype(BF16)
        send(raws.at[n], landing(n, 0), k_fin[n][0], far)

    def finish(n):
        for m in range(2):
            arrive(landing(n, m), k_fin[n][m])

    for i in range(COL_CHUNKS + 1):
        if i < COL_CHUNKS:
            produce(order[i])
        if i:
            spread(order[i - 1])
    for n in order:
        relay(n)
    for n in order:
        finish(n)

    for src, dst, k, dev, when in pending:
        if when is None:
            copy(src, dst, k, dev).wait_send()
        else:
            pl.when(when)(lambda a=(src, dst, k, dev): copy(*a).wait_send())


def vmem(shape, dtype):
    return pltpu.VMEM(shape, dtype)


SCRATCH = [
    vmem((NY * NC, TOK, FEAT), BF16),
    vmem((D, 1024), BF16),
    vmem((16, D), BF16),
    vmem((HEAD + VAL, D), BF16),
    vmem((TOK, 1024), F32),
    vmem((TOK, 128), F32),
    vmem((NX, TOK, HEAD), BF16),
    vmem((NZ, TOK, 2 * HEAD), BF16),
    vmem((NX, TOK, 128), F32),
    vmem((NX, TOK, 128), F32),
    vmem((NX, TOK, 2 * HEAD), F32),
    vmem((NX, TOK, HEAD), BF16),
    vmem((NX, 8, 128), F32),
    vmem((NX, TOK, HEAD), BF16),
    vmem((NX, 8, 128), F32),
    vmem((NX, TOK, HEAD), F32),
    vmem((TOK, 128), F32),
    vmem((TOK, VAL), F32),
    vmem((TOK, 128), BF16),
    vmem((NX, VAL // NX + 16, 128), BF16),
    vmem((NX, VAL // NX + 16, 128), BF16),
    vmem((NZ, VAL // NX + 16, 128), BF16),
    vmem((NX, VAL // NX, 128), BF16),
    vmem((NX, VAL // NX, 128), BF16),
    vmem((TOK, HEAD + VAL), BF16),
    vmem((COL_CHUNKS, NC, NY, 32, COLS), BF16),
    vmem((COL_CHUNKS, NY, 32, COLS), BF16),
    vmem((COL_CHUNKS, NY, 32, COLS), BF16),
    vmem((COL_CHUNKS, 32, COLS), BF16),
    vmem((COL_CHUNKS, 32, COLS), BF16),
    vmem((1, D), F32),
    vmem((1, NZ * NX * TOK), F32),
    vmem((16, HEAD), BF16),
    vmem((1, HEAD), F32),
    vmem((1, VAL), F32),
    pltpu.SemaphoreType.DMA((N_SEM,)),
    pltpu.SemaphoreType.DMA((N_SEM,)),
    pltpu.SemaphoreType.DMA((N_LOC,)),
]


def local(
    tokens,
    norm_gain,
    fox_query,
    fox_key,
    fox_value,
    cum_gate,
    lin_query,
    lin_key,
    lin_value,
    decay_down,
    decay_up,
    decay_bias,
    lin_gain,
    fox_out,
    lin_out,
):
    here = pl.BlockSpec(memory_space=pltpu.VMEM)
    far = pl.BlockSpec(memory_space=pl.ANY)
    own_part, fin, log_total = pl.pallas_call(
        kernel,
        name="layer",
        out_shape=(
            jax.ShapeDtypeStruct((32, D), BF16),
            jax.ShapeDtypeStruct((2, 32, D), BF16),
            jax.ShapeDtypeStruct((1, TOK), F32),
        ),
        in_specs=[far] * 15,
        out_specs=(here, here, here),
        scratch_shapes=SCRATCH,
        compiler_params=pltpu.CompilerParams(
            collective_id=0, has_side_effects=True, vmem_limit_bytes=60 * 1024 * 1024
        ),
    )(
        tokens,
        norm_gain.reshape(1, D),
        fox_query,
        fox_key,
        fox_value,
        cum_gate,
        lin_query,
        lin_key,
        lin_value,
        decay_down.T,
        decay_up,
        decay_bias.reshape(1, HEAD),
        lin_gain.reshape(1, VAL),
        fox_out,
        lin_out,
    )
    mixed = own_part.astype(F32) + fin[0].astype(F32) + fin[1].astype(F32)
    return mixed.astype(BF16), log_total


def solution(mesh):
    torus = Mesh(mesh.devices.reshape(NZ, NX, NY, NC), ("z", "x", "y", "c"))
    sp, tp, sp_tp = ("z", "x"), ("y", "c"), ("z", "x", "y", "c")
    in_specs = (
        P(sp, tp),
        P(),
        P(None, tp),
        P(None, tp),
        P(None, tp),
        P(tp, None),
        P(None, tp),
        P(None, tp),
        P(None, tp),
        P(),
        P(None, tp),
        P(tp),
        P(),
        P(tp, None),
        P(tp, None),
    )
    out_specs = (P(sp_tp, None), P(tp, sp))
    return jax.shard_map(local, mesh=torus, in_specs=in_specs, out_specs=out_specs, check_vma=False)
```

```python
import jax
import jax.numpy as jnp
from jax import lax
from jax.experimental import pallas as pl
from jax.experimental.pallas import tpu as pltpu
from jax.sharding import Mesh
from jax.sharding import PartitionSpec as P

MESH = pl.DeviceIdType.MESH
F32 = jnp.float32
BF16 = jnp.bfloat16

NZ, NX, NY, NC = 8, 4, 4, 2
TOK = 256
D = 4096
FEAT = 512
HEAD = 128
VAL = 256
EPS = 1e-06
TAU = 16.0
LOW = -3.0e38
KEY_SCALE = 128 ** (-0.5)

CHUNKS = 4
ROWS = TOK // CHUNKS
KV_CHUNKS = 4
KV_ROWS = TOK // KV_CHUNKS
COL_CHUNKS = 8
COLS = D // COL_CHUNKS
N_SEM = 160
GROUP_DOWN, GROUP_OWN, GROUP_UP = 0, 1, 2
N_LOC = 16


def nt(a, b):
    return lax.dot_general(a, b, (((1,), (1,)), ((), ())), preferred_element_type=F32)


def tn(a, b):
    return lax.dot_general(a, b, (((0,), (0,)), ((), ())), preferred_element_type=F32)


def mm(a, b):
    return jnp.dot(a, b, preferred_element_type=F32)


def iota(shape, dim):
    return lax.broadcasted_iota(jnp.int32, shape, dim)


def column_of(row):
    eye = iota((128, 128), 0) == iota((128, 128), 1)
    return jnp.sum(jnp.where(eye, row, 0.0), axis=1, keepdims=True)


def row_of(square):
    eye = iota((128, 128), 0) == iota((128, 128), 1)
    return jnp.sum(jnp.where(eye, square, 0.0), axis=0, keepdims=True)


def split3(value):
    high = value.astype(BF16)
    rest = value - high.astype(F32)
    mid = rest.astype(BF16)
    low = (rest - mid.astype(F32)).astype(BF16)
    return high, mid, low


def kernel(
    tokens,
    norm_gain_far,
    fox_query,
    fox_key,
    fox_value,
    cum_gate_far,
    lin_query,
    lin_key,
    lin_value,
    decay_down,
    decay_up_far,
    decay_bias_far,
    lin_gain_far,
    fox_out,
    lin_out,
    own_part,
    fin,
    log_total,
    xg,
    w,
    wd,
    wo,
    acc,
    ssq,
    qs,
    kv,
    cq,
    top,
    oacc,
    ob,
    lb,
    op,
    lp,
    share,
    lh,
    lcum,
    lout,
    qext,
    s1s,
    s1,
    s2,
    s3s,
    s3,
    heads,
    cb,
    far_rows,
    raw,
    raws,
    norm_gain,
    cum_gate,
    decay_up,
    decay_bias,
    lin_gain,
    ss,
    rs,
    ls,
):
    z, x = lax.axis_index("z"), lax.axis_index("x")
    y, c = lax.axis_index("y"), lax.axis_index("c")
    other = 1 - c
    yp, ym, yo = lax.rem(y + 1, NY), lax.rem(y + 3, NY), lax.rem(y + 2, NY)
    zp, zm = lax.rem(z + 1, NZ), lax.rem(z + 7, NZ)
    sib = (z, x, y, other)
    up, down = (z, x, yp, c), (z, x, ym, c)
    z_up, z_down = (zp, x, y, c), (zm, x, y, c)

    sites = [0]
    pending = []

    def site():
        sites[0] += 1
        return sites[0] - 1

    def copy(src, dst, k, dev):
        return pltpu.make_async_remote_copy(
            src_ref=src,
            dst_ref=dst,
            send_sem=ss.at[k],
            recv_sem=rs.at[k],
            device_id=dev,
            device_id_type=MESH,
        )

    def send(src, dst, k, dev, when=None):
        if when is None:
            copy(src, dst, k, dev).start()
        else:
            pl.when(when)(lambda: copy(src, dst, k, dev).start())
        pending.append((src, dst, k, dev, when))

    def arrive(dst, k):
        copy(dst, dst, k, sib).wait_recv()

    own = y * 2 + c
    first = pltpu.make_async_copy(tokens, xg.at[own], ls.at[0])
    first.start()
    weights = []
    column = 0
    for n, ref in enumerate((fox_query, fox_key, fox_value, lin_query, lin_key, lin_value)):
        width = ref.shape[1]
        weights.append(pltpu.make_async_copy(ref, w.at[:, pl.ds(column, width)], ls.at[1 + n]))
        column += width
    weights.append(pltpu.make_async_copy(decay_down, wd, ls.at[7]))
    smalls = [
        pltpu.make_async_copy(norm_gain_far, norm_gain, ls.at[10]),
        pltpu.make_async_copy(cum_gate_far, cum_gate, ls.at[11]),
        pltpu.make_async_copy(decay_up_far, decay_up, ls.at[12]),
        pltpu.make_async_copy(decay_bias_far, decay_bias, ls.at[13]),
        pltpu.make_async_copy(lin_gain_far, lin_gain, ls.at[14]),
    ]
    weights = smalls + weights
    for item in weights:
        item.start()
    outs = [
        pltpu.make_async_copy(fox_out, wo.at[pl.ds(0, HEAD), :], ls.at[8]),
        pltpu.make_async_copy(lin_out, wo.at[pl.ds(HEAD, VAL), :], ls.at[9]),
    ]
    for item in outs:
        item.start()

    partners = [sib, up, down]
    partners += [(z, lax.rem(x + n, NX), y, core) for n in range(1, NX) for core in (c, other)]
    z_four = (lax.rem(z + 4, NZ), x, y, c)
    partners += [z_up, z_down, z_four]
    barrier = pltpu.get_barrier_semaphore()
    for dev in partners:
        pl.semaphore_signal(barrier, inc=1, device_id=dev, device_id_type=MESH)
    pl.semaphore_wait(barrier, len(partners))

    first.wait()
    k_sib = site()
    k_up = [site() for _ in range(CHUNKS)]
    k_down = [site() for _ in range(CHUNKS)]
    k_far = [site() for _ in range(CHUNKS)]
    k_relay = [[site() for _ in range(CHUNKS)] for _ in range(3)]
    half = CHUNKS // 2

    def piece(block, n):
        return xg.at[block, pl.ds(n * ROWS, ROWS), :]

    def push(block, n, k, dev):
        send(piece(block, n), piece(block, n), k, dev)

    for n in range(CHUNKS):
        push(own, n, k_up[n], up)
        m = (n + half) % CHUNKS
        push(own, m, k_down[m], down)
    send(xg.at[own], xg.at[own], k_sib, sib)

    b_m, b_p, b_o = ym * 2 + c, yp * 2 + c, yo * 2 + c
    for item in weights:
        item.wait()

    def widen(i, _):
        rows = pl.ds(pl.multiple_of(i * FEAT, FEAT), FEAT)
        part = jnp.concatenate([wd[:, rows].astype(F32), jnp.zeros((112, FEAT), F32)], axis=0)
        w[rows, pl.ds(896, 128)] = part.T.astype(BF16)

    lax.fori_loop(0, NY * NC, widen, None)
    acc[...] = jnp.zeros_like(acc)
    ssq[...] = jnp.zeros_like(ssq)

    def project(block, start=0, width=1024):
        xb = xg[block].astype(F32)
        if start == 0:
            ssq[...] += jnp.sum(xb * xb, axis=1, keepdims=True)
        rows = pl.multiple_of(block * FEAT, FEAT)
        gain = norm_gain[:, pl.ds(rows, FEAT)]
        cols = pl.ds(start, width)
        acc[:, cols] += mm((xb * gain).astype(BF16), w[pl.ds(rows, FEAT), cols])

    project(own)
    for n in range(half):
        m = n + half
        arrive(piece(b_m, n), k_up[n])
        push(b_m, n, k_far[n], up)
        push(b_m, n, k_relay[0][n], sib)
        arrive(piece(b_p, m), k_down[m])
        push(b_p, m, k_far[m], down)
        push(b_p, m, k_relay[1][m], sib)
    s_own, s_m, s_p, s_o = y * 2 + other, ym * 2 + other, yp * 2 + other, yo * 2 + other
    arrive(xg.at[s_own], k_sib)
    project(s_own)
    for n in range(half):
        m = n + half
        arrive(piece(b_m, m), k_up[m])
        push(b_m, m, k_relay[0][m], sib)
        arrive(piece(b_p, n), k_down[n])
        push(b_p, n, k_relay[1][n], sib)
    project(b_m)
    project(b_p)
    late_blocks = (s_m, s_p)
    for n in range(half):
        m = n + half
        arrive(piece(b_o, n), k_far[n])
        push(b_o, n, k_relay[2][n], sib)
        arrive(piece(b_o, m), k_far[m])
        push(b_o, m, k_relay[2][m], sib)
        if n < 2:
            for r in range(CHUNKS):
                arrive(piece(late_blocks[n], r), k_relay[n][r])
            project(late_blocks[n])
    project(b_o)
    for n in range(CHUNKS):
        arrive(piece(s_o, n), k_relay[2][n])
    project(s_o, 0, 512)

    norm = lax.rsqrt(ssq[:, 0:1] * (1.0 / D) + EPS)

    def result(start, width):
        return acc[:, pl.ds(start, width)] * norm

    qs[x] = (result(0, 128) * HEAD ** (-0.5)).astype(BF16)
    kv[z] = result(128, 256).astype(BF16)

    kv_half = KV_CHUNKS // 2

    def reach(n):
        return (4, 3) if n < KV_CHUNKS - 1 else (3, 4)

    k_kv = {}
    for step in range(1, 5):
        for n in range(KV_CHUNKS):
            for way in (0, 1):
                if step <= reach(n)[way]:
                    k_kv[step, n, way] = site()

    def origin(step, way):
        return lax.rem(z + (NZ - step if way == 0 else step), NZ)

    def kv_piece(block, n):
        return kv.at[block, pl.ds(n * KV_ROWS, KV_ROWS), :]

    def wanted(step, n, way, receiver):
        if way == 0:
            return receiver >= step
        far = receiver + step
        return jnp.logical_or(far >= NZ, far + 1 <= reach(n)[1])

    def kv_send(step, n, way):
        if (step, n, way) in k_kv:
            part = kv_piece(origin(step - 1, way), n)
            dev, receiver = (z_down, zm) if way else (z_up, zp)
            send(part, part, k_kv[step, n, way], dev, wanted(step, n, way, receiver))

    def kv_step(step, n, way):
        if (step, n, way) in k_kv:
            part = kv_piece(origin(step, way), n)
            k = k_kv[step, n, way]
            pl.when(wanted(step, n, way, z))(lambda: arrive(part, k))
            kv_send(step + 1, n, way)

    def slot(step, number):
        m = number % kv_half
        pairs = ((m, 0), (m + kv_half, 1)) if number < kv_half else ((m + kv_half, 0), (m, 1))
        for n, way in pairs:
            kv_step(step, n, way)

    for m in range(kv_half):
        kv_send(1, m, 0)
        kv_send(1, m + kv_half, 1)
    for m in range(kv_half):
        kv_send(1, m + kv_half, 0)
        kv_send(1, m, 1)

    def x_at(n):
        return lax.rem(x + n, NX)

    project(s_o, 512, 512)

    k_wo = [site(), site()]
    send(fox_out, wo.at[pl.ds(HEAD + VAL, HEAD), :], k_wo[0], sib)
    send(lin_out, wo.at[pl.ds(2 * HEAD + VAL, VAL), :], k_wo[1], sib)

    lk = result(512, 128).astype(BF16).astype(F32)
    lv = result(640, 256).astype(BF16)
    low = result(896, 128).astype(BF16)
    up_weight = jnp.concatenate([decay_up[...], jnp.zeros((112, 128), BF16)], axis=0)
    pre = mm(low, up_weight) + decay_bias[...]
    decay = (jnp.minimum(pre, 0.0) - jnp.log1p(jnp.exp(-jnp.abs(pre)))) * (1.0 / TAU)
    lower = (iota((TOK, TOK), 0) >= iota((TOK, TOK), 1)).astype(BF16)
    sums = mm(lower, jnp.concatenate(split3(decay), axis=1))
    cum = sums[:, 0:128] + sums[:, 128:256] + sums[:, 256:384]
    lcum[...] = cum
    last = cum[TOK - 1 : TOK, :]
    state = tn(lv, (lk * jnp.exp(last - cum)).astype(BF16))
    quarter = VAL // NX
    row16 = iota((16, 128), 0)

    def pack(ref, values, total):
        ref[pl.ds(0, quarter), :] = values.astype(BF16)
        parts = split3(total)
        tail = jnp.zeros((16, 128), F32)
        for n in range(3):
            tail = jnp.where(row16 == n, parts[n].astype(F32), tail)
        ref[pl.ds(quarter, 16), :] = tail.astype(BF16)

    def unpack(ref):
        values = ref[pl.ds(0, quarter), :].astype(F32)
        tail = ref[pl.ds(quarter, 16), :].astype(F32)
        total = tail[0:1, :] + tail[1:2, :] + tail[2:3, :]
        return values, total

    for n in range(NX):
        pack(s1s.at[n], state[n * quarter : (n + 1) * quarter, :], last)
    k_s1 = [site() for _ in range(NX)]
    for n in range(1, NX):
        send(s1s.at[x_at(n)], s1.at[x], k_s1[n], (z, x_at(n), y, c))

    k_q = [site() for _ in range(NX)]
    for n in range(1, NX):
        send(qs.at[x], qs.at[x], k_q[n], (z, x_at(n), y, c))

    lq = result(384, 128).astype(BF16).astype(F32) * KEY_SCALE
    qext[...] = (lq * jnp.exp(cum)).astype(BF16)
    rows_i, cols_j = iota((TOK, TOK), 0), iota((TOK, TOK), 1)
    row_id = iota((TOK, HEAD), 0)
    grouped = (TOK // 8, 8, HEAD)
    q8, k8, c8 = lq.reshape(grouped), lk.reshape(grouped), cum.reshape(grouped)
    place = iota(grouped, 1)
    total = jnp.zeros((TOK, TOK), F32)
    for back in range(8):
        if back:
            gap = jnp.where(place >= back, c8 - pltpu.roll(c8, back, 1), -jnp.inf)
            product = q8 * pltpu.roll(k8, back, 1) * jnp.exp(gap)
        else:
            product = q8 * k8
        one = jnp.sum(product.reshape(TOK, HEAD), axis=1, keepdims=True)
        total = jnp.where(rows_i - cols_j == back, one, total)
    span = 8
    while span < TOK:
        pairs = (TOK // (2 * span), 2 * span, HEAD)
        edge = jnp.broadcast_to(cum.reshape(pairs)[:, span - 1 : span, :], pairs).reshape(TOK, HEAD)
        right = (row_id // span) % 2 == 1
        fall = jnp.exp(-jnp.abs(cum - edge))
        q_part = jnp.where(right, lq * fall, 0.0).astype(BF16)
        k_part = jnp.where(right, 0.0, lk * fall).astype(BF16)
        same = rows_i // (2 * span) == cols_j // (2 * span)
        total = total + jnp.where(same, nt(q_part, k_part), 0.0)
        span *= 2
    lout[...] = mm(total.astype(BF16), lv)

    for j in range(NX):
        for n in range(2):
            start = pl.multiple_of((z * NX + j) * TOK + n * 128, 128)
            column_gate = column_of(cum_gate[:, pl.ds(start, 128)])
            cq[j, pl.ds(n * 128, 128), :] = jnp.broadcast_to(column_gate, (128, 128))

    def logits(j, block):
        start = pl.multiple_of((block * NX + x) * TOK, TOK)
        gate = cum_gate[:, pl.ds(start, TOK)]
        own_gate = cq[j]
        own_gate = jnp.concatenate([own_gate, own_gate], axis=1)
        return nt(qs[j], kv[block, :, pl.ds(0, HEAD)]) + (own_gate - gate)

    def values(block):
        return jnp.concatenate(
            [kv[block, :, pl.ds(HEAD, HEAD)], jnp.ones((TOK, HEAD), BF16)], axis=1
        )

    def diagonal(some):
        mine = values(z)
        for j in some:
            seen = iota((TOK, TOK), 1) + x * TOK <= iota((TOK, TOK), 0) + j * TOK
            logit = jnp.where(seen, logits(j, z), LOW)
            peak = jnp.max(logit, axis=1, keepdims=True)
            top[j] = jnp.broadcast_to(peak, (TOK, HEAD))
            oacc[j] = mm(jnp.exp(logit - peak).astype(BF16), mine)

    def update(block, some):
        theirs = values(block)
        for j in some:
            logit = logits(j, block)
            old = top[j]
            peak = jnp.maximum(old, jnp.max(logit, axis=1, keepdims=True))
            top[j] = peak
            wide = jnp.concatenate([peak, peak], axis=1)
            weight = jnp.exp(logit - wide).astype(BF16)
            fade = jnp.exp(old - peak)
            fade = jnp.concatenate([fade, fade], axis=1)
            oacc[j] = oacc[j] * fade + mm(weight, theirs)

    def attend(step, way):
        block = origin(step, way)
        pl.when(block < z)(lambda: update(block, range(NX)))

    slot(1, 0)
    slot(1, 1)

    for n in range(1, NX):
        arrive(s1.at[x_at(NX - n)], k_s1[n])
    s1[x] = s1s[x]
    row_state, row_total = jnp.zeros((quarter, 128), F32), jnp.zeros((1, 128), F32)
    for n in range(NX):
        values_n, total_n = unpack(s1.at[n])
        row_state = jnp.exp(total_n) * row_state + values_n
        row_total = row_total + total_n
    pack(s2.at[z], row_state, row_total)
    k_s2 = {(step, way): site() for step in range(1, 4) for way in (0, 1)}
    k_far_state = site()

    def state_send(step, way):
        if (step, way) in k_s2:
            dev, receiver = (z_down, zm) if way else (z_up, zp)
            part = s2.at[origin(step - 1, way)]
            send(part, part, k_s2[step, way], dev, wanted(step, 0, way, receiver))

    def state_step(step):
        for way in (0, 1):
            if (step, way) in k_s2:
                part, k = s2.at[origin(step, way)], k_s2[step, way]
                pl.when(wanted(step, 0, way, z))(lambda part=part, k=k: arrive(part, k))
                state_send(step + 1, way)

    state_send(1, 0)
    state_send(1, 1)
    send(s2.at[z], s2.at[z], k_far_state, z_four, z < 4)

    slot(1, 2)
    slot(1, 3)
    diagonal([x])
    slot(2, 0)
    slot(2, 1)
    state_step(1)
    for n in range(1, NX):
        arrive(qs.at[x_at(NX - n)], k_q[n])
    diagonal([x_at(n) for n in range(1, NX)])
    slot(2, 2)
    attend(1, 0)
    slot(2, 3)
    attend(1, 1)
    attend(2, 0)
    state_step(2)
    slot(3, 0)
    slot(3, 1)
    attend(2, 1)
    slot(3, 2)
    slot(3, 3)
    attend(3, 0)

    state_step(3)
    far_state = s2.at[lax.rem(z + 4, NZ)]
    pl.when(z >= 4)(lambda: arrive(far_state, k_far_state))

    def earlier(n, state):
        values_n, total_n = unpack(s2.at[n])
        return jnp.exp(total_n) * state + values_n

    state = lax.fori_loop(0, z, earlier, jnp.zeros((quarter, 128), F32))
    for n in range(NX):
        s3s[n] = state.astype(BF16)
        values_n, total_n = unpack(s1.at[n])
        state = jnp.exp(total_n) * state + values_n
    k_s3 = [site() for _ in range(NX)]
    for n in range(1, NX):
        send(s3s.at[x_at(n)], s3.at[x], k_s3[n], (z, x_at(n), y, c))

    slot(4, 0)
    slot(4, 1)
    attend(3, 1)
    slot(4, 2)
    slot(4, 3)

    k_o = [[site(), site()] for _ in range(NX)]
    k_rest = [[site(), site()] for _ in range(NX)]
    rest = pl.ds(1, NY - 1)
    k_l = [[site(), site()] for _ in range(NX)]
    row8 = iota((8, 128), 0)
    cores = (c, other)

    def of_core(value, core):
        parts = value.reshape(NY, NC, 32, value.shape[1])
        return parts[:, core].reshape(TOK // 2, value.shape[1])

    def keep(ref, value):
        for n in range(NY):
            ref[lax.rem(n + NY - yo, NY)] = value[n * 32 : (n + 1) * 32]


    for pair in ((2, 1), (3, 0)):
        some = [x_at(n) for n in pair]
        pl.when(z >= 4)(lambda some=some: update(origin(4, 0), some))
        for n, j in zip(pair, some):
            mass = oacc[j][:, HEAD:]
            height = top[j] + jnp.log(mass)
            row = [row_of(of_core(height, core)) for core in range(NC)]
            lp[j] = jnp.where(row8 == 0, row[0], jnp.where(row8 == 1, row[1], 0.0))
            result_j = (oacc[j][:, 0:HEAD] / mass).astype(BF16)
            for core in range(NC):
                keep(op.at[j, core], of_core(result_j, core))
            for h in range(2):
                if n or h:
                    dev = (z, j, y, cores[h])
                    send(lp.at[j], lb.at[h, x], k_l[n][h], dev)
                    send(op.at[j, cores[h], 0], ob.at[h, x, 0], k_o[n][h], dev)
    for n in (2, 1, 3, 0):
        for h in range(2):
            if n or h:
                dev = (z, x_at(n), y, cores[h])
                part = op.at[x_at(n), cores[h], rest]
                send(part, ob.at[h, x, rest], k_rest[n][h], dev)

    for n in range(1, NX):
        arrive(s3.at[x_at(NX - n)], k_s3[n])
    s3[x] = s3s[x]
    whole = jnp.concatenate([s3[n] for n in range(NX)], axis=0)
    lin_raw = lout[...] + nt(qext[...], whole)
    mean = jnp.mean(lin_raw * lin_raw, axis=1, keepdims=True)
    lin_done = (lin_raw * lax.rsqrt(mean + EPS) * lin_gain[...]).astype(BF16)
    for core in range(NC):
        keep(lh.at[core], of_core(lin_done, core))
    k_lh = site()
    lin_there = heads.at[:, :, pl.ds(2 * HEAD + VAL, VAL)]
    send(lh.at[other], lin_there, k_lh, sib)
    heads[:, :, pl.ds(HEAD, VAL)] = lh[c]

    for n in range(NX):
        for h in range(2):
            if n or h:
                arrive(lb.at[h, x_at(NX - n)], k_l[n][h])
    lb[0, x] = lp[x]
    ob[0, x] = op[x, c]
    summit = None
    for h in range(2):
        heights = [lb[h, n] for n in range(NX)]
        peak = jnp.maximum(
            jnp.maximum(heights[0], heights[1]), jnp.maximum(heights[2], heights[3])
        )
        shares = [jnp.exp(height - peak) for height in heights]
        mass = shares[0] + shares[1] + shares[2] + shares[3]
        if h == 0:
            summit = peak + jnp.log(mass)
        for m in range(NX):
            even = (shares[m] / mass)[0:2, :]
            mine_row = jnp.where(c == 0, even[0:1, :], even[1:2, :])
            keep(share.at[h, m], jnp.broadcast_to(column_of(mine_row), (128, HEAD)))
    parts = []
    for n in range(NY):
        for core in range(NC):
            parts.append(summit[core : core + 1, n * 32 : (n + 1) * 32])
    log_total[...] = jnp.concatenate(parts, axis=1)
    for item in outs:
        item.wait()
    arrive(wo.at[pl.ds(HEAD + VAL, HEAD), :], k_wo[0])
    arrive(wo.at[pl.ds(2 * HEAD + VAL, VAL), :], k_wo[1])
    arrive(lin_there, k_lh)
    def landing(n, m):
        return fin.at[m, :, pl.ds(n * COLS, COLS)]

    k_raw = [site() for _ in range(COL_CHUNKS)]
    k_fin = [[site() for _ in range(2)] for _ in range(COL_CHUNKS)]
    col_half = COL_CHUNKS // 2
    order = [n + half_n for n in range(col_half) for half_n in (0, col_half)]

    def ways(n):
        return (up, GROUP_UP, down, GROUP_DOWN) if n < col_half else (down, GROUP_DOWN, up, GROUP_UP)

    def wait_parts(keys, groups):
        for n in range(NX):
            for h in range(2):
                if n or h:
                    arrive(ob.at[h, x_at(NX - n), groups], keys[n][h])

    def mix(groups):
        for h in range(2):
            total = share[h, 0, groups] * ob[h, 0, groups].astype(F32)
            for m in range(1, NX):
                total = total + share[h, m, groups] * ob[h, m, groups].astype(F32)
            heads[groups, :, pl.ds(h * (HEAD + VAL), HEAD)] = total.astype(BF16)

    wait_parts(k_o, 0)
    mix(0)
    for n in order:
        far_rows[n] = mm(heads[0], wo[:, pl.ds(n * COLS, COLS)]).astype(BF16)
        send(far_rows.at[n], raw.at[n], k_raw[n], ways(n)[0])
    wait_parts(k_rest, rest)
    mix(rest)

    def direct(n):
        left = heads[rest].reshape(96, 2 * (HEAD + VAL))
        part = mm(left, wo[:, pl.ds(n * COLS, COLS)])
        cb[n] = part.astype(BF16).reshape(NY - 1, 32, COLS)
        near, group = ways(n)[2:]
        send(cb.at[n, group], landing(n, 1), k_fin[n][1], near)

    def relay(n):
        arrive(raw.at[n], k_raw[n])
        far, group = ways(n)[:2]
        raws[n] = (cb[n, group].astype(F32) + raw[n].astype(F32)).astype(BF16)
        send(raws.at[n], landing(n, 0), k_fin[n][0], far)

    def finish(n):
        for m in range(2):
            arrive(landing(n, m), k_fin[n][m])

    for n in order:
        direct(n)
    for n in range(COL_CHUNKS):
        own_part[:, pl.ds(n * COLS, COLS)] = cb[n, GROUP_OWN]
    for n in order:
        relay(n)
    for n in order:
        finish(n)

    for src, dst, k, dev, when in pending:
        if when is None:
            copy(src, dst, k, dev).wait_send()
        else:
            pl.when(when)(lambda a=(src, dst, k, dev): copy(*a).wait_send())


def finish_kernel(own_part, fin, log_in, mixed, log_out):
    total = own_part[...].astype(F32) + fin[0].astype(F32) + fin[1].astype(F32)
    mixed[...] = total.astype(BF16)
    log_out[...] = log_in[...]


def vmem(shape, dtype):
    return pltpu.VMEM(shape, dtype)


SCRATCH = [
    vmem((NY * NC, TOK, FEAT), BF16),
    vmem((D, 1024), BF16),
    vmem((16, D), BF16),
    vmem((2 * (HEAD + VAL), D), BF16),
    vmem((TOK, 1024), F32),
    vmem((TOK, 128), F32),
    vmem((NX, TOK, HEAD), BF16),
    vmem((NZ, TOK, 2 * HEAD), BF16),
    vmem((NX, TOK, 128), F32),
    vmem((NX, TOK, 128), F32),
    vmem((NX, TOK, 2 * HEAD), F32),
    vmem((2, NX, NY, 32, HEAD), BF16),
    vmem((2, NX, 8, 128), F32),
    vmem((NX, NC, NY, 32, HEAD), BF16),
    vmem((NX, 8, 128), F32),
    vmem((2, NX, NY, 32, HEAD), F32),
    vmem((NC, NY, 32, VAL), BF16),
    vmem((TOK, 128), F32),
    vmem((TOK, VAL), F32),
    vmem((TOK, 128), BF16),
    vmem((NX, VAL // NX + 16, 128), BF16),
    vmem((NX, VAL // NX + 16, 128), BF16),
    vmem((NZ, VAL // NX + 16, 128), BF16),
    vmem((NX, VAL // NX, 128), BF16),
    vmem((NX, VAL // NX, 128), BF16),
    vmem((NY, 32, 2 * (HEAD + VAL)), BF16),
    vmem((COL_CHUNKS, NY - 1, 32, COLS), BF16),
    vmem((COL_CHUNKS, 32, COLS), BF16),
    vmem((COL_CHUNKS, 32, COLS), BF16),
    vmem((COL_CHUNKS, 32, COLS), BF16),
    vmem((1, D), F32),
    vmem((1, NZ * NX * TOK), F32),
    vmem((16, HEAD), BF16),
    vmem((1, HEAD), F32),
    vmem((1, VAL), F32),
    pltpu.SemaphoreType.DMA((N_SEM,)),
    pltpu.SemaphoreType.DMA((N_SEM,)),
    pltpu.SemaphoreType.DMA((N_LOC,)),
]


def local(
    tokens,
    norm_gain,
    fox_query,
    fox_key,
    fox_value,
    cum_gate,
    lin_query,
    lin_key,
    lin_value,
    decay_down,
    decay_up,
    decay_bias,
    lin_gain,
    fox_out,
    lin_out,
):
    here = pl.BlockSpec(memory_space=pltpu.VMEM)
    far = pl.BlockSpec(memory_space=pl.ANY)
    own_part, fin, log_total = pl.pallas_call(
        kernel,
        name="layer",
        out_shape=(
            jax.ShapeDtypeStruct((32, D), BF16),
            jax.ShapeDtypeStruct((2, 32, D), BF16),
            jax.ShapeDtypeStruct((1, TOK), F32),
        ),
        in_specs=[far] * 15,
        out_specs=(here, here, here),
        scratch_shapes=SCRATCH,
        compiler_params=pltpu.CompilerParams(
            collective_id=0, has_side_effects=True, vmem_limit_bytes=60 * 1024 * 1024
        ),
    )(
        tokens,
        norm_gain.reshape(1, D),
        fox_query,
        fox_key,
        fox_value,
        cum_gate,
        lin_query,
        lin_key,
        lin_value,
        decay_down.T,
        decay_up,
        decay_bias.reshape(1, HEAD),
        lin_gain.reshape(1, VAL),
        fox_out,
        lin_out,
    )
    return pl.pallas_call(
        finish_kernel,
        name="finish",
        out_shape=(
            jax.ShapeDtypeStruct((32, D), BF16),
            jax.ShapeDtypeStruct((1, TOK), F32),
        ),
        in_specs=[here] * 3,
        out_specs=(here, here),
    )(own_part, fin, log_total)


def solution(mesh):
    torus = Mesh(mesh.devices.reshape(NZ, NX, NY, NC), ("z", "x", "y", "c"))
    sp, tp, sp_tp = ("z", "x"), ("y", "c"), ("z", "x", "y", "c")
    in_specs = (
        P(sp, tp),
        P(),
        P(None, tp),
        P(None, tp),
        P(None, tp),
        P(tp, None),
        P(None, tp),
        P(None, tp),
        P(None, tp),
        P(),
        P(None, tp),
        P(tp),
        P(),
        P(tp, None),
        P(tp, None),
    )
    out_specs = (P(sp_tp, None), P(tp, sp))
    return jax.shard_map(local, mesh=torus, in_specs=in_specs, out_specs=out_specs, check_vma=False)
```

```python
import jax
import jax.numpy as jnp
from jax import lax
from jax.experimental import pallas as pl
from jax.experimental.pallas import tpu as pltpu
from jax.sharding import Mesh
from jax.sharding import PartitionSpec as P

MESH = pl.DeviceIdType.MESH
F32 = jnp.float32
BF16 = jnp.bfloat16

NZ, NX, NY, NC = 8, 4, 4, 2
TOK = 256
D = 4096
FEAT = 512
HEAD = 128
VAL = 256
EPS = 1e-06
TAU = 16.0
LOW = -3.0e38
KEY_SCALE = 128 ** (-0.5)

CHUNKS = 4
ROWS = TOK // CHUNKS
KV_CHUNKS = 4
KV_ROWS = TOK // KV_CHUNKS
COL_CHUNKS = 8
COLS = D // COL_CHUNKS
N_SEM = 160
GROUP_DOWN, GROUP_OWN, GROUP_UP = 0, 1, 2
N_LOC = 16


def nt(a, b):
    return lax.dot_general(a, b, (((1,), (1,)), ((), ())), preferred_element_type=F32)


def tn(a, b):
    return lax.dot_general(a, b, (((0,), (0,)), ((), ())), preferred_element_type=F32)


def mm(a, b):
    return jnp.dot(a, b, preferred_element_type=F32)


def iota(shape, dim):
    return lax.broadcasted_iota(jnp.int32, shape, dim)


def column_of(row):
    eye = iota((128, 128), 0) == iota((128, 128), 1)
    return jnp.sum(jnp.where(eye, row, 0.0), axis=1, keepdims=True)


def row_of(square):
    eye = iota((128, 128), 0) == iota((128, 128), 1)
    return jnp.sum(jnp.where(eye, square, 0.0), axis=0, keepdims=True)


def split3(value):
    high = value.astype(BF16)
    rest = value - high.astype(F32)
    mid = rest.astype(BF16)
    low = (rest - mid.astype(F32)).astype(BF16)
    return high, mid, low


def kernel(
    tokens,
    norm_gain_far,
    fox_query,
    fox_key,
    fox_value,
    cum_gate_far,
    lin_query,
    lin_key,
    lin_value,
    decay_down,
    decay_up_far,
    decay_bias_far,
    lin_gain_far,
    fox_out,
    lin_out,
    mixed,
    log_total,
    xg,
    w,
    wd,
    wo,
    acc,
    ssq,
    qs,
    kv,
    cq,
    top,
    oacc,
    ob,
    lb,
    op,
    lp,
    share,
    lh,
    lcum,
    lout,
    qext,
    s1s,
    s1,
    s2,
    s3s,
    s3,
    heads,
    cb,
    far_rows,
    raw,
    raws,
    fin,
    norm_gain,
    cum_gate,
    decay_up,
    decay_bias,
    lin_gain,
    ss,
    rs,
    ls,
):
    z, x = lax.axis_index("z"), lax.axis_index("x")
    y, c = lax.axis_index("y"), lax.axis_index("c")
    other = 1 - c
    yp, ym, yo = lax.rem(y + 1, NY), lax.rem(y + 3, NY), lax.rem(y + 2, NY)
    zp, zm = lax.rem(z + 1, NZ), lax.rem(z + 7, NZ)
    sib = (z, x, y, other)
    up, down = (z, x, yp, c), (z, x, ym, c)
    z_up, z_down = (zp, x, y, c), (zm, x, y, c)

    sites = [0]
    pending = []

    def site():
        sites[0] += 1
        return sites[0] - 1

    def copy(src, dst, k, dev):
        return pltpu.make_async_remote_copy(
            src_ref=src,
            dst_ref=dst,
            send_sem=ss.at[k],
            recv_sem=rs.at[k],
            device_id=dev,
            device_id_type=MESH,
        )

    def send(src, dst, k, dev, when=None):
        if when is None:
            copy(src, dst, k, dev).start()
        else:
            pl.when(when)(lambda: copy(src, dst, k, dev).start())
        pending.append((src, dst, k, dev, when))

    def arrive(dst, k):
        copy(dst, dst, k, sib).wait_recv()

    own = y * 2 + c
    first = pltpu.make_async_copy(tokens, xg.at[own], ls.at[0])
    first.start()
    partners = [sib, up, down]
    partners += [(z, lax.rem(x + n, NX), y, core) for n in range(1, NX) for core in (c, other)]
    z_four = (lax.rem(z + 4, NZ), x, y, c)
    partners += [z_up, z_down, z_four]
    barrier = pltpu.get_barrier_semaphore()
    for dev in partners:
        pl.semaphore_signal(barrier, inc=1, device_id=dev, device_id_type=MESH)
    weights = []
    column = 0
    for n, ref in enumerate((fox_query, fox_key, fox_value, lin_query, lin_key, lin_value)):
        width = ref.shape[1]
        weights.append(pltpu.make_async_copy(ref, w.at[:, pl.ds(column, width)], ls.at[1 + n]))
        column += width
    weights.append(pltpu.make_async_copy(decay_down, wd, ls.at[7]))
    smalls = [
        pltpu.make_async_copy(norm_gain_far, norm_gain, ls.at[10]),
        pltpu.make_async_copy(cum_gate_far, cum_gate, ls.at[11]),
        pltpu.make_async_copy(decay_up_far, decay_up, ls.at[12]),
        pltpu.make_async_copy(decay_bias_far, decay_bias, ls.at[13]),
        pltpu.make_async_copy(lin_gain_far, lin_gain, ls.at[14]),
    ]
    weights = smalls + weights
    for item in weights:
        item.start()
    outs = [
        pltpu.make_async_copy(fox_out, wo.at[pl.ds(0, HEAD), :], ls.at[8]),
        pltpu.make_async_copy(lin_out, wo.at[pl.ds(HEAD, VAL), :], ls.at[9]),
    ]

    pl.semaphore_wait(barrier, len(partners))

    first.wait()
    k_sib = site()
    k_up = [site() for _ in range(CHUNKS)]
    k_down = [site() for _ in range(CHUNKS)]
    k_far = [site() for _ in range(CHUNKS)]
    k_relay = [[site() for _ in range(CHUNKS)] for _ in range(3)]
    half = CHUNKS // 2

    def piece(block, n):
        return xg.at[block, pl.ds(n * ROWS, ROWS), :]

    def push(block, n, k, dev):
        send(piece(block, n), piece(block, n), k, dev)

    for n in range(CHUNKS):
        push(own, n, k_up[n], up)
        m = (n + half) % CHUNKS
        push(own, m, k_down[m], down)
    send(xg.at[own], xg.at[own], k_sib, sib)

    b_m, b_p, b_o = ym * 2 + c, yp * 2 + c, yo * 2 + c
    for item in weights:
        item.wait()

    def widen(i, _):
        rows = pl.ds(pl.multiple_of(i * FEAT, FEAT), FEAT)
        part = jnp.concatenate([wd[:, rows].astype(F32), jnp.zeros((112, FEAT), F32)], axis=0)
        w[rows, pl.ds(896, 128)] = part.T.astype(BF16)

    lax.fori_loop(0, NY * NC, widen, None)
    acc[...] = jnp.zeros_like(acc)
    ssq[...] = jnp.zeros_like(ssq)

    def project(block, start=0, width=1024):
        xb = xg[block].astype(F32)
        if start == 0:
            ssq[...] += jnp.sum(xb * xb, axis=1, keepdims=True)
        rows = pl.multiple_of(block * FEAT, FEAT)
        gain = norm_gain[:, pl.ds(rows, FEAT)]
        cols = pl.ds(start, width)
        acc[:, cols] += mm((xb * gain).astype(BF16), w[pl.ds(rows, FEAT), cols])

    project(own)
    for n in range(half):
        m = n + half
        arrive(piece(b_m, n), k_up[n])
        push(b_m, n, k_far[n], up)
        push(b_m, n, k_relay[0][n], sib)
        arrive(piece(b_p, m), k_down[m])
        push(b_p, m, k_far[m], down)
        push(b_p, m, k_relay[1][m], sib)
    s_own, s_m, s_p, s_o = y * 2 + other, ym * 2 + other, yp * 2 + other, yo * 2 + other
    arrive(xg.at[s_own], k_sib)
    project(s_own)
    for n in range(half):
        m = n + half
        arrive(piece(b_m, m), k_up[m])
        push(b_m, m, k_relay[0][m], sib)
        arrive(piece(b_p, n), k_down[n])
        push(b_p, n, k_relay[1][n], sib)
    project(b_m)
    project(b_p)
    late_blocks = (s_m, s_p)
    for n in range(half):
        m = n + half
        arrive(piece(b_o, n), k_far[n])
        push(b_o, n, k_relay[2][n], sib)
        arrive(piece(b_o, m), k_far[m])
        push(b_o, m, k_relay[2][m], sib)
        if n < 2:
            for r in range(CHUNKS):
                arrive(piece(late_blocks[n], r), k_relay[n][r])
            project(late_blocks[n])
    project(b_o)
    for n in range(CHUNKS):
        arrive(piece(s_o, n), k_relay[2][n])
    project(s_o, 0, 512)

    norm = lax.rsqrt(ssq[:, 0:1] * (1.0 / D) + EPS)

    def result(start, width):
        return acc[:, pl.ds(start, width)] * norm

    qs[x] = (result(0, 128) * HEAD ** (-0.5)).astype(BF16)
    kv[z] = result(128, 256).astype(BF16)

    kv_half = KV_CHUNKS // 2

    def reach(n):
        return (4, 3) if n < KV_CHUNKS - 1 else (3, 4)

    k_kv = {}
    for step in range(1, 5):
        for n in range(KV_CHUNKS):
            for way in (0, 1):
                if step <= reach(n)[way]:
                    k_kv[step, n, way] = site()

    def origin(step, way):
        return lax.rem(z + (NZ - step if way == 0 else step), NZ)

    def kv_piece(block, n):
        return kv.at[block, pl.ds(n * KV_ROWS, KV_ROWS), :]

    def wanted(step, n, way, receiver):
        if way == 0:
            return receiver >= step
        far = receiver + step
        return jnp.logical_or(far >= NZ, far + 1 <= reach(n)[1])

    def kv_send(step, n, way):
        if (step, n, way) in k_kv:
            part = kv_piece(origin(step - 1, way), n)
            dev, receiver = (z_down, zm) if way else (z_up, zp)
            send(part, part, k_kv[step, n, way], dev, wanted(step, n, way, receiver))

    def kv_step(step, n, way):
        if (step, n, way) in k_kv:
            part = kv_piece(origin(step, way), n)
            k = k_kv[step, n, way]
            pl.when(wanted(step, n, way, z))(lambda: arrive(part, k))
            kv_send(step + 1, n, way)

    def slot(step, number):
        m = number % kv_half
        pairs = ((m, 0), (m + kv_half, 1)) if number < kv_half else ((m + kv_half, 0), (m, 1))
        for n, way in pairs:
            kv_step(step, n, way)

    for m in range(kv_half):
        kv_send(1, m, 0)
        kv_send(1, m + kv_half, 1)
    for m in range(kv_half):
        kv_send(1, m + kv_half, 0)
        kv_send(1, m, 1)

    def x_at(n):
        return lax.rem(x + n, NX)

    project(s_o, 512, 512)

    for item in outs:
        item.start()
    k_wo = [site(), site()]
    send(fox_out, wo.at[pl.ds(HEAD + VAL, HEAD), :], k_wo[0], sib)
    send(lin_out, wo.at[pl.ds(2 * HEAD + VAL, VAL), :], k_wo[1], sib)

    lk = result(512, 128).astype(BF16).astype(F32)
    lv = result(640, 256).astype(BF16)
    low = result(896, 128).astype(BF16)
    up_weight = jnp.concatenate([decay_up[...], jnp.zeros((112, 128), BF16)], axis=0)
    pre = mm(low, up_weight) + decay_bias[...]
    decay = (jnp.minimum(pre, 0.0) - jnp.log1p(jnp.exp(-jnp.abs(pre)))) * (1.0 / TAU)
    lower = (iota((TOK, TOK), 0) >= iota((TOK, TOK), 1)).astype(BF16)
    sums = mm(lower, jnp.concatenate(split3(decay), axis=1))
    cum = sums[:, 0:128] + sums[:, 128:256] + sums[:, 256:384]
    lcum[...] = cum
    last = cum[TOK - 1 : TOK, :]
    state = tn(lv, (lk * jnp.exp(last - cum)).astype(BF16))
    quarter = VAL // NX
    row16 = iota((16, 128), 0)

    def pack(ref, values, total):
        ref[pl.ds(0, quarter), :] = values.astype(BF16)
        parts = split3(total)
        tail = jnp.zeros((16, 128), F32)
        for n in range(3):
            tail = jnp.where(row16 == n, parts[n].astype(F32), tail)
        ref[pl.ds(quarter, 16), :] = tail.astype(BF16)

    def unpack(ref):
        values = ref[pl.ds(0, quarter), :].astype(F32)
        tail = ref[pl.ds(quarter, 16), :].astype(F32)
        total = tail[0:1, :] + tail[1:2, :] + tail[2:3, :]
        return values, total

    for n in range(NX):
        pack(s1s.at[n], state[n * quarter : (n + 1) * quarter, :], last)
    k_s1 = [site() for _ in range(NX)]
    for n in range(1, NX):
        send(s1s.at[x_at(n)], s1.at[x], k_s1[n], (z, x_at(n), y, c))

    k_q = [site() for _ in range(NX)]
    for n in range(1, NX):
        send(qs.at[x], qs.at[x], k_q[n], (z, x_at(n), y, c))

    lq = result(384, 128).astype(BF16).astype(F32) * KEY_SCALE
    qext[...] = (lq * jnp.exp(cum)).astype(BF16)
    rows_i, cols_j = iota((TOK, TOK), 0), iota((TOK, TOK), 1)
    row_id = iota((TOK, HEAD), 0)
    grouped = (TOK // 8, 8, HEAD)
    q8, k8, c8 = lq.reshape(grouped), lk.reshape(grouped), cum.reshape(grouped)
    place = iota(grouped, 1)
    total = jnp.zeros((TOK, TOK), F32)
    for back in range(8):
        if back:
            gap = jnp.where(place >= back, c8 - pltpu.roll(c8, back, 1), -jnp.inf)
            product = q8 * pltpu.roll(k8, back, 1) * jnp.exp(gap)
        else:
            product = q8 * k8
        one = jnp.sum(product.reshape(TOK, HEAD), axis=1, keepdims=True)
        total = jnp.where(rows_i - cols_j == back, one, total)
    span = 8
    while span < TOK:
        pairs = (TOK // (2 * span), 2 * span, HEAD)
        edge = jnp.broadcast_to(cum.reshape(pairs)[:, span - 1 : span, :], pairs).reshape(TOK, HEAD)
        right = (row_id // span) % 2 == 1
        fall = jnp.exp(-jnp.abs(cum - edge))
        q_part = jnp.where(right, lq * fall, 0.0).astype(BF16)
        k_part = jnp.where(right, 0.0, lk * fall).astype(BF16)
        same = rows_i // (2 * span) == cols_j // (2 * span)
        total = total + jnp.where(same, nt(q_part, k_part), 0.0)
        span *= 2
    lout[...] = mm(total.astype(BF16), lv)

    for j in range(NX):
        for n in range(2):
            start = pl.multiple_of((z * NX + j) * TOK + n * 128, 128)
            column_gate = column_of(cum_gate[:, pl.ds(start, 128)])
            cq[j, pl.ds(n * 128, 128), :] = jnp.broadcast_to(column_gate, (128, 128))

    def logits(j, block):
        start = pl.multiple_of((block * NX + x) * TOK, TOK)
        gate = cum_gate[:, pl.ds(start, TOK)]
        own_gate = cq[j]
        own_gate = jnp.concatenate([own_gate, own_gate], axis=1)
        return nt(qs[j], kv[block, :, pl.ds(0, HEAD)]) + (own_gate - gate)

    def values(block):
        return jnp.concatenate(
            [kv[block, :, pl.ds(HEAD, HEAD)], jnp.ones((TOK, HEAD), BF16)], axis=1
        )

    def diagonal(some):
        mine = values(z)
        for j in some:
            seen = iota((TOK, TOK), 1) + x * TOK <= iota((TOK, TOK), 0) + j * TOK
            logit = jnp.where(seen, logits(j, z), LOW)
            peak = jnp.max(logit, axis=1, keepdims=True)
            top[j] = jnp.broadcast_to(peak, (TOK, HEAD))
            oacc[j] = mm(jnp.exp(logit - peak).astype(BF16), mine)

    def update(block, some):
        theirs = values(block)
        for j in some:
            logit = logits(j, block)
            old = top[j]
            peak = jnp.maximum(old, jnp.max(logit, axis=1, keepdims=True))
            top[j] = peak
            wide = jnp.concatenate([peak, peak], axis=1)
            weight = jnp.exp(logit - wide).astype(BF16)
            fade = jnp.exp(old - peak)
            fade = jnp.concatenate([fade, fade], axis=1)
            oacc[j] = oacc[j] * fade + mm(weight, theirs)

    def attend(step, way):
        block = origin(step, way)
        pl.when(block < z)(lambda: update(block, range(NX)))

    slot(1, 0)
    slot(1, 1)

    for n in range(1, NX):
        arrive(s1.at[x_at(NX - n)], k_s1[n])
    s1[x] = s1s[x]
    row_state, row_total = jnp.zeros((quarter, 128), F32), jnp.zeros((1, 128), F32)
    for n in range(NX):
        values_n, total_n = unpack(s1.at[n])
        row_state = jnp.exp(total_n) * row_state + values_n
        row_total = row_total + total_n
    pack(s2.at[z], row_state, row_total)
    k_s2 = {(step, way): site() for step in range(1, 4) for way in (0, 1)}
    k_far_state = site()

    def state_send(step, way):
        if (step, way) in k_s2:
            dev, receiver = (z_down, zm) if way else (z_up, zp)
            part = s2.at[origin(step - 1, way)]
            send(part, part, k_s2[step, way], dev, wanted(step, 0, way, receiver))

    def state_step(step):
        for way in (0, 1):
            if (step, way) in k_s2:
                part, k = s2.at[origin(step, way)], k_s2[step, way]
                pl.when(wanted(step, 0, way, z))(lambda part=part, k=k: arrive(part, k))
                state_send(step + 1, way)

    state_send(1, 0)
    state_send(1, 1)
    send(s2.at[z], s2.at[z], k_far_state, z_four, z < 4)

    slot(1, 2)
    slot(1, 3)
    diagonal([x])
    slot(2, 0)
    slot(2, 1)
    state_step(1)
    for n in range(1, NX):
        arrive(qs.at[x_at(NX - n)], k_q[n])
    diagonal([x_at(n) for n in range(1, NX)])
    slot(2, 2)
    attend(1, 0)
    slot(2, 3)
    attend(1, 1)
    attend(2, 0)
    state_step(2)
    slot(3, 0)
    slot(3, 1)
    attend(2, 1)
    slot(3, 2)
    slot(3, 3)
    attend(3, 0)

    state_step(3)
    far_state = s2.at[lax.rem(z + 4, NZ)]
    pl.when(z >= 4)(lambda: arrive(far_state, k_far_state))

    def earlier(n, state):
        values_n, total_n = unpack(s2.at[n])
        return jnp.exp(total_n) * state + values_n

    state = lax.fori_loop(0, z, earlier, jnp.zeros((quarter, 128), F32))
    for n in range(NX):
        s3s[n] = state.astype(BF16)
        values_n, total_n = unpack(s1.at[n])
        state = jnp.exp(total_n) * state + values_n
    k_s3 = [site() for _ in range(NX)]
    for n in range(1, NX):
        send(s3s.at[x_at(n)], s3.at[x], k_s3[n], (z, x_at(n), y, c))

    attend(3, 1)
    slot(4, 0)
    slot(4, 1)
    slot(4, 2)
    slot(4, 3)

    k_o = [[site(), site()] for _ in range(NX)]
    k_rest = [[site(), site()] for _ in range(NX)]
    rest = pl.ds(1, NY - 1)
    k_l = [[site(), site()] for _ in range(NX)]
    row8 = iota((8, 128), 0)
    cores = (c, other)

    def of_core(value, core):
        parts = value.reshape(NY, NC, 32, value.shape[1])
        return parts[:, core].reshape(TOK // 2, value.shape[1])

    def keep(ref, value):
        for n in range(NY):
            ref[lax.rem(n + NY - yo, NY)] = value[n * 32 : (n + 1) * 32]


    for pair in ((2, 1, 3, 0),):
        some = [x_at(n) for n in pair]
        pl.when(z >= 4)(lambda some=some: update(origin(4, 0), some))
        for n, j in zip(pair, some):
            mass = oacc[j][:, HEAD:]
            height = top[j] + jnp.log(mass)
            row = [row_of(of_core(height, core)) for core in range(NC)]
            lp[j] = jnp.where(row8 == 0, row[0], jnp.where(row8 == 1, row[1], 0.0))
            result_j = (oacc[j][:, 0:HEAD] / mass).astype(BF16)
            for core in range(NC):
                keep(op.at[j, core], of_core(result_j, core))
            for h in range(2):
                if n or h:
                    dev = (z, j, y, cores[h])
                    send(lp.at[j], lb.at[h, x], k_l[n][h], dev)
                    send(op.at[j, cores[h], 0], ob.at[h, x, 0], k_o[n][h], dev)
    for n in (2, 1, 3, 0):
        for h in range(2):
            if n or h:
                dev = (z, x_at(n), y, cores[h])
                part = op.at[x_at(n), cores[h], rest]
                send(part, ob.at[h, x, rest], k_rest[n][h], dev)

    for n in range(1, NX):
        arrive(s3.at[x_at(NX - n)], k_s3[n])
    s3[x] = s3s[x]
    whole = jnp.concatenate([s3[n] for n in range(NX)], axis=0)
    lin_raw = lout[...] + nt(qext[...], whole)
    mean = jnp.mean(lin_raw * lin_raw, axis=1, keepdims=True)
    lin_done = (lin_raw * lax.rsqrt(mean + EPS) * lin_gain[...]).astype(BF16)
    for core in range(NC):
        keep(lh.at[core], of_core(lin_done, core))
    k_lh = site()
    lin_there = heads.at[:, :, pl.ds(2 * HEAD + VAL, VAL)]
    send(lh.at[other], lin_there, k_lh, sib)
    heads[:, :, pl.ds(HEAD, VAL)] = lh[c]

    for n in range(NX):
        for h in range(2):
            if n or h:
                arrive(lb.at[h, x_at(NX - n)], k_l[n][h])
    lb[0, x] = lp[x]
    ob[0, x] = op[x, c]
    summit = None
    share_rows = {}
    for h in range(2):
        heights = [lb[h, n] for n in range(NX)]
        peak = jnp.maximum(
            jnp.maximum(heights[0], heights[1]), jnp.maximum(heights[2], heights[3])
        )
        shares = [jnp.exp(height - peak) for height in heights]
        mass = shares[0] + shares[1] + shares[2] + shares[3]
        if h == 0:
            summit = peak + jnp.log(mass)
        for m in range(NX):
            even = shares[m] / mass
            share_rows[h, m] = jnp.where(c == 0, even[0:1, :], even[1:2, :])

    def columns(group):
        place = iota((32, 128), 0) + lax.rem(yo + group, NY) * 32
        for h in range(2):
            for m in range(NX):
                picked = jnp.where(iota((32, 128), 1) == place, share_rows[h, m], 0.0)
                column = jnp.sum(picked, axis=1, keepdims=True)
                share[h, m, group] = jnp.broadcast_to(column, (32, HEAD))

    columns(0)
    for item in outs:
        item.wait()
    arrive(wo.at[pl.ds(HEAD + VAL, HEAD), :], k_wo[0])
    arrive(wo.at[pl.ds(2 * HEAD + VAL, VAL), :], k_wo[1])
    arrive(lin_there, k_lh)
    def landing(n, m):
        return fin.at[m, :, pl.ds(n * COLS, COLS)]

    k_raw = [site() for _ in range(COL_CHUNKS)]
    k_fin = [[site() for _ in range(2)] for _ in range(COL_CHUNKS)]
    col_half = COL_CHUNKS // 2
    order = [n + half_n for n in range(col_half) for half_n in (0, col_half)]

    def ways(n):
        return (up, GROUP_UP, down, GROUP_DOWN) if n < col_half else (down, GROUP_DOWN, up, GROUP_UP)

    def wait_parts(keys, groups):
        for n in range(NX):
            for h in range(2):
                if n or h:
                    arrive(ob.at[h, x_at(NX - n), groups], keys[n][h])

    def mix(groups):
        for h in range(2):
            total = share[h, 0, groups] * ob[h, 0, groups].astype(F32)
            for m in range(1, NX):
                total = total + share[h, m, groups] * ob[h, m, groups].astype(F32)
            heads[groups, :, pl.ds(h * (HEAD + VAL), HEAD)] = total.astype(BF16)

    wait_parts(k_o, 0)
    mix(0)
    for n in order:
        far_rows[n] = mm(heads[0], wo[:, pl.ds(n * COLS, COLS)]).astype(BF16)
        send(far_rows.at[n], raw.at[n], k_raw[n], ways(n)[0])
    parts = []
    for n in range(NY):
        for core in range(NC):
            parts.append(summit[core : core + 1, n * 32 : (n + 1) * 32])
    log_total[...] = jnp.concatenate(parts, axis=1)
    for group in range(1, NY):
        columns(group)
    wait_parts(k_rest, rest)
    mix(rest)

    def direct(n):
        left = heads[rest].reshape(96, 2 * (HEAD + VAL))
        part = mm(left, wo[:, pl.ds(n * COLS, COLS)])
        cb[n] = part.astype(BF16).reshape(NY - 1, 32, COLS)
        near, group = ways(n)[2:]
        send(cb.at[n, group], landing(n, 1), k_fin[n][1], near)

    def relay(n):
        arrive(raw.at[n], k_raw[n])
        far, group = ways(n)[:2]
        raws[n] = (cb[n, group].astype(F32) + raw[n].astype(F32)).astype(BF16)
        send(raws.at[n], landing(n, 0), k_fin[n][0], far)

    def finish(n):
        for m in range(2):
            arrive(landing(n, m), k_fin[n][m])
        cols = pl.ds(n * COLS, COLS)
        done = cb[n, GROUP_OWN].astype(F32) + fin[0, :, cols].astype(F32)
        mixed[:, cols] = (done + fin[1, :, cols].astype(F32)).astype(BF16)

    for n in order:
        direct(n)
    for n in order:
        relay(n)
    for n in order:
        finish(n)

    for src, dst, k, dev, when in pending:
        if when is None:
            copy(src, dst, k, dev).wait_send()
        else:
            pl.when(when)(lambda a=(src, dst, k, dev): copy(*a).wait_send())


def finish_kernel(mixed_in, log_in, mixed_out, log_out):
    mixed_out[...] = mixed_in[...]
    log_out[...] = log_in[...]


def vmem(shape, dtype):
    return pltpu.VMEM(shape, dtype)


SCRATCH = [
    vmem((NY * NC, TOK, FEAT), BF16),
    vmem((D, 1024), BF16),
    vmem((16, D), BF16),
    vmem((2 * (HEAD + VAL), D), BF16),
    vmem((TOK, 1024), F32),
    vmem((TOK, 128), F32),
    vmem((NX, TOK, HEAD), BF16),
    vmem((NZ, TOK, 2 * HEAD), BF16),
    vmem((NX, TOK, 128), F32),
    vmem((NX, TOK, 128), F32),
    vmem((NX, TOK, 2 * HEAD), F32),
    vmem((2, NX, NY, 32, HEAD), BF16),
    vmem((2, NX, 8, 128), F32),
    vmem((NX, NC, NY, 32, HEAD), BF16),
    vmem((NX, 8, 128), F32),
    vmem((2, NX, NY, 32, HEAD), F32),
    vmem((NC, NY, 32, VAL), BF16),
    vmem((TOK, 128), F32),
    vmem((TOK, VAL), F32),
    vmem((TOK, 128), BF16),
    vmem((NX, VAL // NX + 16, 128), BF16),
    vmem((NX, VAL // NX + 16, 128), BF16),
    vmem((NZ, VAL // NX + 16, 128), BF16),
    vmem((NX, VAL // NX, 128), BF16),
    vmem((NX, VAL // NX, 128), BF16),
    vmem((NY, 32, 2 * (HEAD + VAL)), BF16),
    vmem((COL_CHUNKS, NY - 1, 32, COLS), BF16),
    vmem((COL_CHUNKS, 32, COLS), BF16),
    vmem((COL_CHUNKS, 32, COLS), BF16),
    vmem((COL_CHUNKS, 32, COLS), BF16),
    vmem((2, 32, D), BF16),
    vmem((1, D), F32),
    vmem((1, NZ * NX * TOK), F32),
    vmem((16, HEAD), BF16),
    vmem((1, HEAD), F32),
    vmem((1, VAL), F32),
    pltpu.SemaphoreType.DMA((N_SEM,)),
    pltpu.SemaphoreType.DMA((N_SEM,)),
    pltpu.SemaphoreType.DMA((N_LOC,)),
]


def local(
    tokens,
    norm_gain,
    fox_query,
    fox_key,
    fox_value,
    cum_gate,
    lin_query,
    lin_key,
    lin_value,
    decay_down,
    decay_up,
    decay_bias,
    lin_gain,
    fox_out,
    lin_out,
):
    here = pl.BlockSpec(memory_space=pltpu.VMEM)
    far = pl.BlockSpec(memory_space=pl.ANY)
    mixed, log_total = pl.pallas_call(
        kernel,
        name="layer",
        out_shape=(
            jax.ShapeDtypeStruct((32, D), BF16),
            jax.ShapeDtypeStruct((1, TOK), F32),
        ),
        in_specs=[far] * 15,
        out_specs=(here, here),
        scratch_shapes=SCRATCH,
        compiler_params=pltpu.CompilerParams(
            collective_id=0, has_side_effects=True, vmem_limit_bytes=60 * 1024 * 1024
        ),
    )(
        tokens,
        norm_gain.reshape(1, D),
        fox_query,
        fox_key,
        fox_value,
        cum_gate,
        lin_query,
        lin_key,
        lin_value,
        decay_down.T,
        decay_up,
        decay_bias.reshape(1, HEAD),
        lin_gain.reshape(1, VAL),
        fox_out,
        lin_out,
    )
    return pl.pallas_call(
        finish_kernel,
        name="finish",
        out_shape=(
            jax.ShapeDtypeStruct((32, D), BF16),
            jax.ShapeDtypeStruct((1, TOK), F32),
        ),
        in_specs=[here] * 2,
        out_specs=(here, here),
    )(mixed, log_total)


def solution(mesh):
    torus = Mesh(mesh.devices.reshape(NZ, NX, NY, NC), ("z", "x", "y", "c"))
    sp, tp, sp_tp = ("z", "x"), ("y", "c"), ("z", "x", "y", "c")
    in_specs = (
        P(sp, tp),
        P(),
        P(None, tp),
        P(None, tp),
        P(None, tp),
        P(tp, None),
        P(None, tp),
        P(None, tp),
        P(None, tp),
        P(),
        P(None, tp),
        P(tp),
        P(),
        P(tp, None),
        P(tp, None),
    )
    out_specs = (P(sp_tp, None), P(tp, sp))
    return jax.shard_map(local, mesh=torus, in_specs=in_specs, out_specs=out_specs, check_vma=False)
```

```python
import jax
import jax.numpy as jnp
from jax import lax
from jax.experimental import pallas as pl
from jax.experimental.pallas import tpu as pltpu
from jax.sharding import Mesh
from jax.sharding import PartitionSpec as P

MESH = pl.DeviceIdType.MESH
F32 = jnp.float32
BF16 = jnp.bfloat16

NZ, NX, NY, NC = 8, 4, 4, 2
TOK = 256
D = 4096
FEAT = 512
HEAD = 128
VAL = 256
EPS = 1e-06
TAU = 16.0
LOW = -3.0e38
KEY_SCALE = 128 ** (-0.5)

CHUNKS = 4
ROWS = TOK // CHUNKS
KV_CHUNKS = 4
KV_ROWS = TOK // KV_CHUNKS
COL_CHUNKS = 8
COLS = D // COL_CHUNKS
N_SEM = 160
GROUP_DOWN, GROUP_OWN, GROUP_UP = 0, 1, 2
N_LOC = 16


def nt(a, b):
    return lax.dot_general(a, b, (((1,), (1,)), ((), ())), preferred_element_type=F32)


def tn(a, b):
    return lax.dot_general(a, b, (((0,), (0,)), ((), ())), preferred_element_type=F32)


def mm(a, b):
    return jnp.dot(a, b, preferred_element_type=F32)


def iota(shape, dim):
    return lax.broadcasted_iota(jnp.int32, shape, dim)


def column_of(row):
    eye = iota((128, 128), 0) == iota((128, 128), 1)
    return jnp.sum(jnp.where(eye, row, 0.0), axis=1, keepdims=True)


def row_of(square):
    eye = iota((128, 128), 0) == iota((128, 128), 1)
    return jnp.sum(jnp.where(eye, square, 0.0), axis=0, keepdims=True)


def split3(value):
    high = value.astype(BF16)
    rest = value - high.astype(F32)
    mid = rest.astype(BF16)
    low = (rest - mid.astype(F32)).astype(BF16)
    return high, mid, low


def kernel(
    tokens,
    norm_gain_far,
    fox_query,
    fox_key,
    fox_value,
    cum_gate_far,
    lin_query,
    lin_key,
    lin_value,
    decay_down,
    decay_up_far,
    decay_bias_far,
    lin_gain_far,
    fox_out,
    lin_out,
    mixed,
    log_total,
    xg,
    w,
    wd,
    wo,
    acc,
    ssq,
    qs,
    kv,
    cq,
    top,
    oacc,
    ob,
    lb,
    op,
    lp,
    share,
    lh,
    lcum,
    lout,
    qext,
    s1s,
    s1,
    s2,
    s3s,
    s3,
    heads,
    cb,
    far_rows,
    raw,
    raws,
    fin,
    norm_gain,
    cum_gate,
    decay_up,
    decay_bias,
    lin_gain,
    ss,
    rs,
    ls,
):
    z, x = lax.axis_index("z"), lax.axis_index("x")
    y, c = lax.axis_index("y"), lax.axis_index("c")
    other = 1 - c
    yp, ym, yo = lax.rem(y + 1, NY), lax.rem(y + 3, NY), lax.rem(y + 2, NY)
    zp, zm = lax.rem(z + 1, NZ), lax.rem(z + 7, NZ)
    sib = (z, x, y, other)
    up, down = (z, x, yp, c), (z, x, ym, c)
    z_up, z_down = (zp, x, y, c), (zm, x, y, c)

    sites = [0]
    pending = []

    def site():
        sites[0] += 1
        return sites[0] - 1

    def copy(src, dst, k, dev):
        return pltpu.make_async_remote_copy(
            src_ref=src,
            dst_ref=dst,
            send_sem=ss.at[k],
            recv_sem=rs.at[k],
            device_id=dev,
            device_id_type=MESH,
        )

    def send(src, dst, k, dev, when=None):
        if when is None:
            copy(src, dst, k, dev).start()
        else:
            pl.when(when)(lambda: copy(src, dst, k, dev).start())
        pending.append((src, dst, k, dev, when))

    def arrive(dst, k):
        copy(dst, dst, k, sib).wait_recv()

    own = y * 2 + c
    first = pltpu.make_async_copy(tokens, xg.at[own], ls.at[0])
    first.start()
    partners = [sib, up, down]
    partners += [(z, lax.rem(x + n, NX), y, core) for n in range(1, NX) for core in (c, other)]
    z_four = (lax.rem(z + 4, NZ), x, y, c)
    partners += [z_up, z_down, z_four]
    barrier = pltpu.get_barrier_semaphore()
    for dev in partners:
        pl.semaphore_signal(barrier, inc=1, device_id=dev, device_id_type=MESH)
    weights = []
    column = 0
    for n, ref in enumerate((fox_query, fox_key, fox_value, lin_query, lin_key, lin_value)):
        width = ref.shape[1]
        weights.append(pltpu.make_async_copy(ref, w.at[:, pl.ds(column, width)], ls.at[1 + n]))
        column += width
    weights.append(pltpu.make_async_copy(decay_down, wd, ls.at[7]))
    smalls = [
        pltpu.make_async_copy(norm_gain_far, norm_gain, ls.at[10]),
        pltpu.make_async_copy(cum_gate_far, cum_gate, ls.at[11]),
        pltpu.make_async_copy(decay_up_far, decay_up, ls.at[12]),
        pltpu.make_async_copy(decay_bias_far, decay_bias, ls.at[13]),
        pltpu.make_async_copy(lin_gain_far, lin_gain, ls.at[14]),
    ]
    weights = smalls + weights
    for item in weights:
        item.start()
    outs = [
        pltpu.make_async_copy(fox_out, wo.at[pl.ds(0, HEAD), :], ls.at[8]),
        pltpu.make_async_copy(lin_out, wo.at[pl.ds(HEAD, VAL), :], ls.at[9]),
    ]

    pl.semaphore_wait(barrier, len(partners))

    first.wait()
    k_sib = site()
    k_up = [site() for _ in range(CHUNKS)]
    k_down = [site() for _ in range(CHUNKS)]
    k_far = [site() for _ in range(CHUNKS)]
    k_relay = [[site() for _ in range(CHUNKS)] for _ in range(3)]
    half = CHUNKS // 2

    def piece(block, n):
        return xg.at[block, pl.ds(n * ROWS, ROWS), :]

    def push(block, n, k, dev):
        send(piece(block, n), piece(block, n), k, dev)

    for n in range(CHUNKS):
        push(own, n, k_up[n], up)
        m = (n + half) % CHUNKS
        push(own, m, k_down[m], down)
    send(xg.at[own], xg.at[own], k_sib, sib)

    b_m, b_p, b_o = ym * 2 + c, yp * 2 + c, yo * 2 + c
    for item in weights:
        item.wait()

    def widen(i, _):
        rows = pl.ds(pl.multiple_of(i * FEAT, FEAT), FEAT)
        part = jnp.concatenate([wd[:, rows].astype(F32), jnp.zeros((112, FEAT), F32)], axis=0)
        w[rows, pl.ds(896, 128)] = part.T.astype(BF16)

    lax.fori_loop(0, NY * NC, widen, None)
    acc[...] = jnp.zeros_like(acc)
    ssq[...] = jnp.zeros_like(ssq)

    def project(block, start=0, width=1024):
        xb = xg[block].astype(F32)
        if start == 0:
            ssq[...] += jnp.sum(xb * xb, axis=1, keepdims=True)
        rows = pl.multiple_of(block * FEAT, FEAT)
        gain = norm_gain[:, pl.ds(rows, FEAT)]
        cols = pl.ds(start, width)
        acc[:, cols] += mm((xb * gain).astype(BF16), w[pl.ds(rows, FEAT), cols])

    project(own)
    for n in range(half):
        m = n + half
        arrive(piece(b_m, n), k_up[n])
        push(b_m, n, k_far[n], up)
        push(b_m, n, k_relay[0][n], sib)
        arrive(piece(b_p, m), k_down[m])
        push(b_p, m, k_far[m], down)
        push(b_p, m, k_relay[1][m], sib)
    s_own, s_m, s_p, s_o = y * 2 + other, ym * 2 + other, yp * 2 + other, yo * 2 + other
    arrive(xg.at[s_own], k_sib)
    project(s_own)
    for n in range(half):
        m = n + half
        arrive(piece(b_m, m), k_up[m])
        push(b_m, m, k_relay[0][m], sib)
        arrive(piece(b_p, n), k_down[n])
        push(b_p, n, k_relay[1][n], sib)
    project(b_m)
    project(b_p)
    late_blocks = (s_m, s_p)
    for n in range(half):
        m = n + half
        arrive(piece(b_o, n), k_far[n])
        push(b_o, n, k_relay[2][n], sib)
        arrive(piece(b_o, m), k_far[m])
        push(b_o, m, k_relay[2][m], sib)
        if n < 2:
            for r in range(CHUNKS):
                arrive(piece(late_blocks[n], r), k_relay[n][r])
            project(late_blocks[n])
    project(b_o)
    for n in range(CHUNKS):
        arrive(piece(s_o, n), k_relay[2][n])
    project(s_o, 0, 512)

    norm = lax.rsqrt(ssq[:, 0:1] * (1.0 / D) + EPS)

    def result(start, width):
        return acc[:, pl.ds(start, width)] * norm

    qs[x] = (result(0, 128) * HEAD ** (-0.5)).astype(BF16)
    kv[z] = result(128, 256).astype(BF16)

    kv_half = KV_CHUNKS // 2

    def reach(n):
        return (4, 3) if n < KV_CHUNKS - 1 else (3, 4)

    k_kv = {}
    for step in range(1, 5):
        for n in range(KV_CHUNKS):
            for way in (0, 1):
                if step <= reach(n)[way]:
                    k_kv[step, n, way] = site()

    def origin(step, way):
        return lax.rem(z + (NZ - step if way == 0 else step), NZ)

    def kv_piece(block, n):
        return kv.at[block, pl.ds(n * KV_ROWS, KV_ROWS), :]

    def wanted(step, n, way, receiver):
        if way == 0:
            return receiver >= step
        far = receiver + step
        return jnp.logical_or(far >= NZ, far + 1 <= reach(n)[1])

    def kv_send(step, n, way):
        if (step, n, way) in k_kv:
            part = kv_piece(origin(step - 1, way), n)
            dev, receiver = (z_down, zm) if way else (z_up, zp)
            send(part, part, k_kv[step, n, way], dev, wanted(step, n, way, receiver))

    def kv_step(step, n, way):
        if (step, n, way) in k_kv:
            part = kv_piece(origin(step, way), n)
            k = k_kv[step, n, way]
            pl.when(wanted(step, n, way, z))(lambda: arrive(part, k))
            kv_send(step + 1, n, way)

    def slot(step, number):
        m = number % kv_half
        pairs = ((m, 0), (m + kv_half, 1)) if number < kv_half else ((m + kv_half, 0), (m, 1))
        for n, way in pairs:
            kv_step(step, n, way)

    for m in range(kv_half):
        kv_send(1, m, 0)
        kv_send(1, m + kv_half, 1)
    for m in range(kv_half):
        kv_send(1, m + kv_half, 0)
        kv_send(1, m, 1)

    def x_at(n):
        return lax.rem(x + n, NX)

    project(s_o, 512, 512)

    lk = result(512, 128).astype(BF16).astype(F32)
    lv = result(640, 256).astype(BF16)
    low = result(896, 128).astype(BF16)
    up_weight = jnp.concatenate([decay_up[...], jnp.zeros((112, 128), BF16)], axis=0)
    pre = mm(low, up_weight) + decay_bias[...]
    decay = (jnp.minimum(pre, 0.0) - jnp.log1p(jnp.exp(-jnp.abs(pre)))) * (1.0 / TAU)
    lower = (iota((TOK, TOK), 0) >= iota((TOK, TOK), 1)).astype(BF16)
    sums = mm(lower, jnp.concatenate(split3(decay), axis=1))
    cum = sums[:, 0:128] + sums[:, 128:256] + sums[:, 256:384]
    lcum[...] = cum
    last = cum[TOK - 1 : TOK, :]
    state = tn(lv, (lk * jnp.exp(last - cum)).astype(BF16))
    quarter = VAL // NX
    row16 = iota((16, 128), 0)

    def pack(ref, values, total):
        ref[pl.ds(0, quarter), :] = values.astype(BF16)
        parts = split3(total)
        tail = jnp.zeros((16, 128), F32)
        for n in range(3):
            tail = jnp.where(row16 == n, parts[n].astype(F32), tail)
        ref[pl.ds(quarter, 16), :] = tail.astype(BF16)

    def unpack(ref):
        values = ref[pl.ds(0, quarter), :].astype(F32)
        tail = ref[pl.ds(quarter, 16), :].astype(F32)
        total = tail[0:1, :] + tail[1:2, :] + tail[2:3, :]
        return values, total

    for n in range(NX):
        pack(s1s.at[n], state[n * quarter : (n + 1) * quarter, :], last)
    k_s1 = [site() for _ in range(NX)]
    for n in range(1, NX):
        send(s1s.at[x_at(n)], s1.at[x], k_s1[n], (z, x_at(n), y, c))

    k_q = [site() for _ in range(NX)]
    for n in range(1, NX):
        send(qs.at[x], qs.at[x], k_q[n], (z, x_at(n), y, c))

    lq = result(384, 128).astype(BF16).astype(F32) * KEY_SCALE
    qext[...] = (lq * jnp.exp(cum)).astype(BF16)
    rows_i, cols_j = iota((TOK, TOK), 0), iota((TOK, TOK), 1)
    row_id = iota((TOK, HEAD), 0)
    grouped = (TOK // 8, 8, HEAD)
    q8, k8, c8 = lq.reshape(grouped), lk.reshape(grouped), cum.reshape(grouped)
    place = iota(grouped, 1)
    total = jnp.zeros((TOK, TOK), F32)
    for back in range(8):
        if back:
            gap = jnp.where(place >= back, c8 - pltpu.roll(c8, back, 1), -jnp.inf)
            product = q8 * pltpu.roll(k8, back, 1) * jnp.exp(gap)
        else:
            product = q8 * k8
        one = jnp.sum(product.reshape(TOK, HEAD), axis=1, keepdims=True)
        total = jnp.where(rows_i - cols_j == back, one, total)
    span = 8
    while span < TOK:
        pairs = (TOK // (2 * span), 2 * span, HEAD)
        edge = jnp.broadcast_to(cum.reshape(pairs)[:, span - 1 : span, :], pairs).reshape(TOK, HEAD)
        right = (row_id // span) % 2 == 1
        fall = jnp.exp(-jnp.abs(cum - edge))
        q_part = jnp.where(right, lq * fall, 0.0).astype(BF16)
        k_part = jnp.where(right, 0.0, lk * fall).astype(BF16)
        same = rows_i // (2 * span) == cols_j // (2 * span)
        total = total + jnp.where(same, nt(q_part, k_part), 0.0)
        span *= 2
    lout[...] = mm(total.astype(BF16), lv)

    for j in range(NX):
        for n in range(2):
            start = pl.multiple_of((z * NX + j) * TOK + n * 128, 128)
            column_gate = column_of(cum_gate[:, pl.ds(start, 128)])
            cq[j, pl.ds(n * 128, 128), :] = jnp.broadcast_to(column_gate, (128, 128))

    def logits(j, block):
        start = pl.multiple_of((block * NX + x) * TOK, TOK)
        gate = cum_gate[:, pl.ds(start, TOK)]
        own_gate = cq[j]
        own_gate = jnp.concatenate([own_gate, own_gate], axis=1)
        return nt(qs[j], kv[block, :, pl.ds(0, HEAD)]) + (own_gate - gate)

    def values(block):
        return jnp.concatenate(
            [kv[block, :, pl.ds(HEAD, HEAD)], jnp.ones((TOK, HEAD), BF16)], axis=1
        )

    def diagonal(some):
        mine = values(z)
        for j in some:
            seen = iota((TOK, TOK), 1) + x * TOK <= iota((TOK, TOK), 0) + j * TOK
            logit = jnp.where(seen, logits(j, z), LOW)
            peak = jnp.max(logit, axis=1, keepdims=True)
            top[j] = jnp.broadcast_to(peak, (TOK, HEAD))
            oacc[j] = mm(jnp.exp(logit - peak).astype(BF16), mine)

    def update(block, some):
        theirs = values(block)
        for j in some:
            logit = logits(j, block)
            old = top[j]
            peak = jnp.maximum(old, jnp.max(logit, axis=1, keepdims=True))
            top[j] = peak
            wide = jnp.concatenate([peak, peak], axis=1)
            weight = jnp.exp(logit - wide).astype(BF16)
            fade = jnp.exp(old - peak)
            fade = jnp.concatenate([fade, fade], axis=1)
            oacc[j] = oacc[j] * fade + mm(weight, theirs)

    def attend(step, way):
        block = origin(step, way)
        pl.when(block < z)(lambda: update(block, range(NX)))

    slot(1, 0)
    slot(1, 1)

    for n in range(1, NX):
        arrive(s1.at[x_at(NX - n)], k_s1[n])
    s1[x] = s1s[x]
    row_state, row_total = jnp.zeros((quarter, 128), F32), jnp.zeros((1, 128), F32)
    for n in range(NX):
        values_n, total_n = unpack(s1.at[n])
        row_state = jnp.exp(total_n) * row_state + values_n
        row_total = row_total + total_n
    pack(s2.at[z], row_state, row_total)
    k_s2 = {(step, way): site() for step in range(1, 4) for way in (0, 1)}
    k_far_state = site()

    def state_send(step, way):
        if (step, way) in k_s2:
            dev, receiver = (z_down, zm) if way else (z_up, zp)
            part = s2.at[origin(step - 1, way)]
            send(part, part, k_s2[step, way], dev, wanted(step, 0, way, receiver))

    def state_step(step):
        for way in (0, 1):
            if (step, way) in k_s2:
                part, k = s2.at[origin(step, way)], k_s2[step, way]
                pl.when(wanted(step, 0, way, z))(lambda part=part, k=k: arrive(part, k))
                state_send(step + 1, way)

    state_send(1, 0)
    state_send(1, 1)
    send(s2.at[z], s2.at[z], k_far_state, z_four, z < 4)

    slot(1, 2)
    slot(1, 3)
    diagonal([x])
    slot(2, 0)
    slot(2, 1)
    state_step(1)
    for n in range(1, NX):
        arrive(qs.at[x_at(NX - n)], k_q[n])
    diagonal([x_at(n) for n in range(1, NX)])
    slot(2, 2)
    attend(1, 0)
    slot(2, 3)
    attend(1, 1)
    for item in outs:
        item.start()
    k_wo = [site(), site()]
    send(fox_out, wo.at[pl.ds(HEAD + VAL, HEAD), :], k_wo[0], sib)
    send(lin_out, wo.at[pl.ds(2 * HEAD + VAL, VAL), :], k_wo[1], sib)
    attend(2, 0)
    state_step(2)
    slot(3, 0)
    slot(3, 1)
    attend(2, 1)
    slot(3, 2)
    slot(3, 3)
    state_step(3)
    far_state = s2.at[lax.rem(z + 4, NZ)]
    pl.when(z >= 4)(lambda: arrive(far_state, k_far_state))

    def earlier(n, state):
        values_n, total_n = unpack(s2.at[n])
        return jnp.exp(total_n) * state + values_n

    state = lax.fori_loop(0, z, earlier, jnp.zeros((quarter, 128), F32))
    for n in range(NX):
        s3s[n] = state.astype(BF16)
        values_n, total_n = unpack(s1.at[n])
        state = jnp.exp(total_n) * state + values_n
    k_s3 = [site() for _ in range(NX)]
    for n in range(1, NX):
        send(s3s.at[x_at(n)], s3.at[x], k_s3[n], (z, x_at(n), y, c))

    attend(3, 0)
    attend(3, 1)
    slot(4, 0)
    slot(4, 1)
    slot(4, 2)
    slot(4, 3)

    k_o = [[site(), site()] for _ in range(NX)]
    k_rest = [[site(), site()] for _ in range(NX)]
    rest = pl.ds(1, NY - 1)
    k_l = [[site(), site()] for _ in range(NX)]
    row8 = iota((8, 128), 0)
    cores = (c, other)

    def of_core(value, core):
        parts = value.reshape(NY, NC, 32, value.shape[1])
        return parts[:, core].reshape(TOK // 2, value.shape[1])

    def keep(ref, value):
        for n in range(NY):
            ref[lax.rem(n + NY - yo, NY)] = value[n * 32 : (n + 1) * 32]


    for pair in ((2, 1, 3, 0),):
        some = [x_at(n) for n in pair]
        pl.when(z >= 4)(lambda some=some: update(origin(4, 0), some))
        for n, j in zip(pair, some):
            mass = oacc[j][:, HEAD:]
            height = top[j] + jnp.log(mass)
            row = [row_of(of_core(height, core)) for core in range(NC)]
            lp[j] = jnp.where(row8 == 0, row[0], jnp.where(row8 == 1, row[1], 0.0))
            result_j = (oacc[j][:, 0:HEAD] / mass).astype(BF16)
            for core in range(NC):
                keep(op.at[j, core], of_core(result_j, core))
            for h in range(2):
                if n or h:
                    dev = (z, j, y, cores[h])
                    send(lp.at[j], lb.at[h, x], k_l[n][h], dev)
                    send(op.at[j, cores[h], 0], ob.at[h, x, 0], k_o[n][h], dev)
    for n in (2, 1, 3, 0):
        for h in range(2):
            if n or h:
                dev = (z, x_at(n), y, cores[h])
                part = op.at[x_at(n), cores[h], rest]
                send(part, ob.at[h, x, rest], k_rest[n][h], dev)

    for n in range(1, NX):
        arrive(s3.at[x_at(NX - n)], k_s3[n])
    s3[x] = s3s[x]
    whole = jnp.concatenate([s3[n] for n in range(NX)], axis=0)
    lin_raw = lout[...] + nt(qext[...], whole)
    mean = jnp.mean(lin_raw * lin_raw, axis=1, keepdims=True)
    lin_done = (lin_raw * lax.rsqrt(mean + EPS) * lin_gain[...]).astype(BF16)
    for core in range(NC):
        keep(lh.at[core], of_core(lin_done, core))
    k_lh = site()
    lin_there = heads.at[:, :, pl.ds(2 * HEAD + VAL, VAL)]
    send(lh.at[other], lin_there, k_lh, sib)
    heads[:, :, pl.ds(HEAD, VAL)] = lh[c]

    for n in range(NX):
        for h in range(2):
            if n or h:
                arrive(lb.at[h, x_at(NX - n)], k_l[n][h])
    lb[0, x] = lp[x]
    ob[0, x] = op[x, c]
    summit = None
    share_rows = {}
    for h in range(2):
        heights = [lb[h, n] for n in range(NX)]
        peak = jnp.maximum(
            jnp.maximum(heights[0], heights[1]), jnp.maximum(heights[2], heights[3])
        )
        shares = [jnp.exp(height - peak) for height in heights]
        mass = shares[0] + shares[1] + shares[2] + shares[3]
        if h == 0:
            summit = peak + jnp.log(mass)
        for m in range(NX):
            even = shares[m] / mass
            share_rows[h, m] = jnp.where(c == 0, even[0:1, :], even[1:2, :])

    def columns(group):
        place = iota((32, 128), 0) + lax.rem(yo + group, NY) * 32
        for h in range(2):
            for m in range(NX):
                picked = jnp.where(iota((32, 128), 1) == place, share_rows[h, m], 0.0)
                column = jnp.sum(picked, axis=1, keepdims=True)
                share[h, m, group] = jnp.broadcast_to(column, (32, HEAD))

    columns(0)
    for item in outs:
        item.wait()
    arrive(wo.at[pl.ds(HEAD + VAL, HEAD), :], k_wo[0])
    arrive(wo.at[pl.ds(2 * HEAD + VAL, VAL), :], k_wo[1])
    arrive(lin_there, k_lh)
    def landing(n, m):
        return fin.at[m, :, pl.ds(n * COLS, COLS)]

    k_raw = [site() for _ in range(COL_CHUNKS)]
    k_fin = [[site() for _ in range(2)] for _ in range(COL_CHUNKS)]
    col_half = COL_CHUNKS // 2
    order = [n + half_n for n in range(col_half) for half_n in (0, col_half)]

    def ways(n):
        return (up, GROUP_UP, down, GROUP_DOWN) if n < col_half else (down, GROUP_DOWN, up, GROUP_UP)

    def wait_parts(keys, groups):
        for n in range(NX):
            for h in range(2):
                if n or h:
                    arrive(ob.at[h, x_at(NX - n), groups], keys[n][h])

    def mix(groups):
        for h in range(2):
            total = share[h, 0, groups] * ob[h, 0, groups].astype(F32)
            for m in range(1, NX):
                total = total + share[h, m, groups] * ob[h, m, groups].astype(F32)
            heads[groups, :, pl.ds(h * (HEAD + VAL), HEAD)] = total.astype(BF16)

    wait_parts(k_o, 0)
    mix(0)
    for n in order:
        far_rows[n] = mm(heads[0], wo[:, pl.ds(n * COLS, COLS)]).astype(BF16)
        send(far_rows.at[n], raw.at[n], k_raw[n], ways(n)[0])
    parts = []
    for n in range(NY):
        for core in range(NC):
            parts.append(summit[core : core + 1, n * 32 : (n + 1) * 32])
    log_total[...] = jnp.concatenate(parts, axis=1)
    for group in range(1, NY):
        columns(group)
    wait_parts(k_rest, rest)
    mix(rest)

    def direct(n):
        left = heads[rest].reshape(96, 2 * (HEAD + VAL))
        part = mm(left, wo[:, pl.ds(n * COLS, COLS)])
        cb[n] = part.astype(BF16).reshape(NY - 1, 32, COLS)
        near, group = ways(n)[2:]
        send(cb.at[n, group], landing(n, 1), k_fin[n][1], near)

    def relay(n):
        arrive(raw.at[n], k_raw[n])
        far, group = ways(n)[:2]
        raws[n] = (cb[n, group].astype(F32) + raw[n].astype(F32)).astype(BF16)
        send(raws.at[n], landing(n, 0), k_fin[n][0], far)

    def finish(n):
        for m in range(2):
            arrive(landing(n, m), k_fin[n][m])
        cols = pl.ds(n * COLS, COLS)
        done = cb[n, GROUP_OWN].astype(F32) + fin[0, :, cols].astype(F32)
        mixed[:, cols] = (done + fin[1, :, cols].astype(F32)).astype(BF16)

    for n in order:
        direct(n)
    for n in order:
        relay(n)
    for n in order:
        finish(n)

    for src, dst, k, dev, when in pending:
        if when is None:
            copy(src, dst, k, dev).wait_send()
        else:
            pl.when(when)(lambda a=(src, dst, k, dev): copy(*a).wait_send())


def finish_kernel(mixed_in, log_in, mixed_out, log_out):
    mixed_out[...] = mixed_in[...]
    log_out[...] = log_in[...]


def vmem(shape, dtype):
    return pltpu.VMEM(shape, dtype)


SCRATCH = [
    vmem((NY * NC, TOK, FEAT), BF16),
    vmem((D, 1024), BF16),
    vmem((16, D), BF16),
    vmem((2 * (HEAD + VAL), D), BF16),
    vmem((TOK, 1024), F32),
    vmem((TOK, 128), F32),
    vmem((NX, TOK, HEAD), BF16),
    vmem((NZ, TOK, 2 * HEAD), BF16),
    vmem((NX, TOK, 128), F32),
    vmem((NX, TOK, 128), F32),
    vmem((NX, TOK, 2 * HEAD), F32),
    vmem((2, NX, NY, 32, HEAD), BF16),
    vmem((2, NX, 8, 128), F32),
    vmem((NX, NC, NY, 32, HEAD), BF16),
    vmem((NX, 8, 128), F32),
    vmem((2, NX, NY, 32, HEAD), F32),
    vmem((NC, NY, 32, VAL), BF16),
    vmem((TOK, 128), F32),
    vmem((TOK, VAL), F32),
    vmem((TOK, 128), BF16),
    vmem((NX, VAL // NX + 16, 128), BF16),
    vmem((NX, VAL // NX + 16, 128), BF16),
    vmem((NZ, VAL // NX + 16, 128), BF16),
    vmem((NX, VAL // NX, 128), BF16),
    vmem((NX, VAL // NX, 128), BF16),
    vmem((NY, 32, 2 * (HEAD + VAL)), BF16),
    vmem((COL_CHUNKS, NY - 1, 32, COLS), BF16),
    vmem((COL_CHUNKS, 32, COLS), BF16),
    vmem((COL_CHUNKS, 32, COLS), BF16),
    vmem((COL_CHUNKS, 32, COLS), BF16),
    vmem((2, 32, D), BF16),
    vmem((1, D), F32),
    vmem((1, NZ * NX * TOK), F32),
    vmem((16, HEAD), BF16),
    vmem((1, HEAD), F32),
    vmem((1, VAL), F32),
    pltpu.SemaphoreType.DMA((N_SEM,)),
    pltpu.SemaphoreType.DMA((N_SEM,)),
    pltpu.SemaphoreType.DMA((N_LOC,)),
]


def local(
    tokens,
    norm_gain,
    fox_query,
    fox_key,
    fox_value,
    cum_gate,
    lin_query,
    lin_key,
    lin_value,
    decay_down,
    decay_up,
    decay_bias,
    lin_gain,
    fox_out,
    lin_out,
):
    here = pl.BlockSpec(memory_space=pltpu.VMEM)
    far = pl.BlockSpec(memory_space=pl.ANY)
    mixed, log_total = pl.pallas_call(
        kernel,
        name="layer",
        out_shape=(
            jax.ShapeDtypeStruct((32, D), BF16),
            jax.ShapeDtypeStruct((1, TOK), F32),
        ),
        in_specs=[far] * 15,
        out_specs=(here, here),
        scratch_shapes=SCRATCH,
        compiler_params=pltpu.CompilerParams(
            collective_id=0, has_side_effects=True, vmem_limit_bytes=60 * 1024 * 1024
        ),
    )(
        tokens,
        norm_gain.reshape(1, D),
        fox_query,
        fox_key,
        fox_value,
        cum_gate,
        lin_query,
        lin_key,
        lin_value,
        decay_down.T,
        decay_up,
        decay_bias.reshape(1, HEAD),
        lin_gain.reshape(1, VAL),
        fox_out,
        lin_out,
    )
    return pl.pallas_call(
        finish_kernel,
        name="finish",
        out_shape=(
            jax.ShapeDtypeStruct((32, D), BF16),
            jax.ShapeDtypeStruct((1, TOK), F32),
        ),
        in_specs=[here] * 2,
        out_specs=(here, here),
    )(mixed, log_total)


def solution(mesh):
    torus = Mesh(mesh.devices.reshape(NZ, NX, NY, NC), ("z", "x", "y", "c"))
    sp, tp, sp_tp = ("z", "x"), ("y", "c"), ("z", "x", "y", "c")
    in_specs = (
        P(sp, tp),
        P(),
        P(None, tp),
        P(None, tp),
        P(None, tp),
        P(tp, None),
        P(None, tp),
        P(None, tp),
        P(None, tp),
        P(),
        P(None, tp),
        P(tp),
        P(),
        P(tp, None),
        P(tp, None),
    )
    out_specs = (P(sp_tp, None), P(tp, sp))
    return jax.shard_map(local, mesh=torus, in_specs=in_specs, out_specs=out_specs, check_vma=False)
```
